32 devices in a mesh: fs: 8 (over z, core), tp: 4 (over y, x).
Axes of the slice: x: 2, y: 2, z: 4, core: 2. Of those that a mesh axis runs over, the one named last changes fastest.
Arguments:
- gate_pre: bfloat16 [8192, 5632], P('fs', 'tp'), may hold values from -6 to 6
- up_pre: bfloat16 [8192, 5632], P('fs', 'tp'), may hold values from -6 to 6
- gate_taps: bfloat16 [3, 5632], replicated, may hold values from -3.5 to 3.5
- up_taps: bfloat16 [3, 5632], replicated, may hold values from -3.5 to 3.5
- down_proj: bfloat16 [5632, 2048], P('tp', 'fs'), may hold values from -0.078125 to 0.078125
- cotangent: bfloat16 [8192, 2048], P(('fs', 'tp')), may hold values from -6 to 6
Outputs:
- gate_grad: bfloat16 [8192, 5632], P('fs', 'tp')
- up_grad: bfloat16 [8192, 5632], P('fs', 'tp')
- down_grad: float32 [5632, 2048], P('tp', 'fs')
- row_norms: float32 [5632], P('tp')
- tap_grads: float32 [2, 3, 5632], replicated
The draws below stay inside these ranges and needn't reach their ends.
All inputs are finite; a program needn't handle non-finite values.
Results may differ from the reference program's by a relative error of at most 0.0042.
Values may be sent and summed in bfloat16 or wider, within the bound.
A program may use at most 128 MiB of HBM per device.

```python
import math
import jax
import jax.numpy as jnp
from jax import lax

D = 2048
FF = 5632
TAPS = 3
TOKENS = 8192
N_TP = 4


def with_spikes(array, own_key, source, target, parts, factor):
    owner, partner = [(jnp.arange(array.shape[position]) // (array.shape[position] // parts)).reshape([-1 if axis == position else 1 for axis in range(array.ndim)]) for position in (source, target)]
    chosen = jax.random.permutation(own_key, parts)[partner]
    strong = (owner == chosen) | (owner == (partner + parts // 2) % parts)
    return jnp.where(strong, factor * array, array)


def steps_of(key, dims, cuts, low, high):
    loudness = 1.0
    for position, parts in cuts:
        heights = jax.random.uniform(jax.random.fold_in(jax.random.fold_in(key, 6), position), (parts,), jnp.float32, low / len(cuts), high / len(cuts))
        loudness = loudness * jnp.repeat(jnp.exp(heights), dims[position] // parts).reshape((-1,) + (1,) * (len(dims) - 1 - position))
    return loudness


def centred(own_key, extent, width, bound, shards=(), dtype=jnp.bfloat16):
    drawn = jax.random.normal(own_key, extent, jnp.float32) * width
    if len(shards) > 0:
        drawn = steps_of(own_key, extent, shards, -0.22, 0.18) * drawn
    return jnp.clip(drawn, min=-bound, max=bound).astype(dtype)


def bell_draw_with(rng, extent, deviation, most, cuts, heavy, held_as=jnp.bfloat16):
    array = deviation * jax.random.normal(rng, extent, jnp.float32)
    if cuts:
        array = array * steps_of(rng, extent, cuts, -0.22, 0.18)
    return jnp.clip(with_spikes(array, jax.random.fold_in(rng, 3), *heavy), -most, most).astype(held_as)


def setup_inputs(seed: int = 0) -> dict:
    key_of = jax.random.split(jax.random.key(seed), 7)
    gate_pre = centred(key_of[0], (TOKENS, FF), 1.0, 6.0, ((0, 8), (1, 4)))
    up_pre = centred(key_of[1], (TOKENS, FF), 1.0, 6.0, ((0, 8), (1, 4)))
    gate_taps = centred(key_of[2], (TAPS, FF), TAPS ** -0.5, 3.5)
    up_taps = centred(key_of[3], (TAPS, FF), TAPS ** -0.5, 3.5)
    down_proj = centred(key_of[4], (FF, D), FF ** -0.5, 0.078125, ((0, 4), (1, 8)))
    cotangent = bell_draw_with(key_of[5], (TOKENS, D), 1.0, 6.0, ((0, 32),), (0, 1, 32, 2.75))
    return dict(gate_pre=gate_pre, up_pre=up_pre, gate_taps=gate_taps, up_taps=up_taps, down_proj=down_proj, cotangent=cotangent)


def block_grads(gate_block, up_block, gate_tap_block, up_tap_block, down_block, cotangent):
    count = gate_block.shape[0]
    reach = TAPS - 1
    gate_taps_f = gate_tap_block.astype(jnp.float32)
    up_taps_f = up_tap_block.astype(jnp.float32)
    gate_padded = jnp.pad(gate_block.astype(jnp.float32), ((reach, 0), (0, 0)))
    up_padded = jnp.pad(up_block.astype(jnp.float32), ((reach, 0), (0, 0)))
    gate_conv = gate_taps_f[0] * gate_padded[0:count]
    up_conv = up_taps_f[0] * up_padded[0:count]
    for offset in range(1, TAPS):
        gate_conv = gate_conv + gate_taps_f[offset] * gate_padded[offset:offset + count]
        up_conv = up_conv + up_taps_f[offset] * up_padded[offset:offset + count]
    gate_sigmoid = jax.nn.sigmoid(gate_conv)
    gate_act = gate_conv * gate_sigmoid
    hidden = (gate_act * up_conv).astype(jnp.bfloat16)
    hidden_grad = jnp.dot(cotangent, down_block.T, preferred_element_type=jnp.float32)
    gate_conv_grad = hidden_grad * up_conv * gate_sigmoid * (1.0 + gate_conv * (1.0 - gate_sigmoid))
    up_conv_grad = hidden_grad * gate_act
    gate_grad_pad = jnp.pad(gate_conv_grad, ((0, reach), (0, 0)))
    up_grad_pad = jnp.pad(up_conv_grad, ((0, reach), (0, 0)))
    gate_grad = gate_taps_f[0] * gate_grad_pad[reach:reach + count]
    up_grad = up_taps_f[0] * up_grad_pad[reach:reach + count]
    for offset in range(1, TAPS):
        lead = reach - offset
        gate_grad = gate_grad + gate_taps_f[offset] * gate_grad_pad[lead:lead + count]
        up_grad = up_grad + up_taps_f[offset] * up_grad_pad[lead:lead + count]
    grad_scale = 1.0 / math.sqrt(TOKENS)
    gate_tap_terms = jnp.stack([lax.optimization_barrier(jnp.sum(gate_conv_grad * gate_padded[offset:offset + count], axis=0)) for offset in range(TAPS)])
    up_tap_terms = jnp.stack([lax.optimization_barrier(jnp.sum(up_conv_grad * up_padded[offset:offset + count], axis=0)) for offset in range(TAPS)])
    tap_terms = jnp.stack([gate_tap_terms, up_tap_terms]) * grad_scale
    down_term = jnp.dot(hidden.T, cotangent, preferred_element_type=jnp.float32) * grad_scale
    norms = lax.optimization_barrier(jnp.sum(down_term * down_term, axis=1)) / down_term.shape[1]
    return (gate_grad.astype(jnp.bfloat16), up_grad.astype(jnp.bfloat16), down_term, norms, tap_terms)

def reference(gate_pre, up_pre, gate_taps, up_taps, down_proj, cotangent):
    channels = FF // N_TP
    gate_blocks = gate_pre.reshape(TOKENS, N_TP, channels).transpose(1, 0, 2)
    up_blocks = up_pre.reshape(TOKENS, N_TP, channels).transpose(1, 0, 2)
    gate_tap_blocks = gate_taps.reshape(TAPS, N_TP, channels).transpose(1, 0, 2)
    up_tap_blocks = up_taps.reshape(TAPS, N_TP, channels).transpose(1, 0, 2)
    down_blocks = down_proj.reshape(N_TP, channels, D)
    gate_grad, up_grad, down_grad, row_norms, tap_grads = lax.map(lambda items: block_grads(items[0], items[1], items[2], items[3], items[4], cotangent), (gate_blocks, up_blocks, gate_tap_blocks, up_tap_blocks, down_blocks))
    gate_grad = gate_grad.transpose(1, 0, 2).reshape(TOKENS, FF)
    up_grad = up_grad.transpose(1, 0, 2).reshape(TOKENS, FF)
    down_grad = down_grad.reshape(FF, D)
    row_norms = row_norms.reshape(FF)
    tap_grads = tap_grads.transpose(1, 2, 0, 3).reshape(2, TAPS, FF)
    return (gate_grad, up_grad, down_grad, row_norms, tap_grads)
```

```python
import functools
import math

import jax
import jax.numpy as jnp
from jax import lax
from jax.experimental import pallas as pl
from jax.experimental.pallas import tpu as pltpu
from jax.sharding import PartitionSpec as P

MESH = pl.DeviceIdType.MESH


def snake(position, width):
    row, column = position // width, position % width
    return row * width + column + (row % 2) * (width - 1 - 2 * column)


def gather_kernel(chips, tps, cot_ref, down_ref, cot_out, down_out, *sems):
    (ring_send, ring_recv, line_send, line_recv, pair_send, pair_recv, local_sem) = sems
    f, q = lax.axis_index("fs"), lax.axis_index("tp")
    z, core = f // 2, f % 2
    width = math.isqrt(tps)
    spot = snake(q, width)
    half_ring = tps // 2
    ring_next = (snake((spot + 1) % tps, width), snake((spot + tps - 1) % tps, width))
    rows = cot_ref.shape[0]
    cols = down_ref.shape[1]
    partner = z * 2 + 1 - core
    behind, ahead = z > 0, z < chips - 1

    barrier = pltpu.get_barrier_semaphore()
    for device in ({"tp": ring_next[0]}, {"tp": ring_next[1]}, {"fs": partner}):
        pl.semaphore_signal(barrier, inc=1, device_id=device, device_id_type=MESH)

    @pl.when(behind)
    def _():
        pl.semaphore_signal(barrier, inc=1, device_id={"fs": f - 2}, device_id_type=MESH)

    @pl.when(ahead)
    def _():
        pl.semaphore_signal(barrier, inc=1, device_id={"fs": f + 2}, device_id_type=MESH)

    pl.semaphore_wait(barrier, 4 + (z + chips - 1) // chips - (z + 1) // chips)

    def cot_rows(owner_spot, way, part):
        owner = snake((owner_spot + 2 * tps) % tps, width)
        if part:
            return pl.ds(owner * rows + way * (rows // 2), rows // 2)
        return pl.ds(owner * rows, rows)

    def ring_copy(step, way):
        sign = 1 - 2 * way
        part = step == half_ring
        where = cot_rows(spot - sign * (step - 1), way, part)
        if step == 1:
            src = cot_ref.at[pl.ds(way * (rows // 2), rows // 2)] if part else cot_ref
        else:
            src = cot_out.at[where]
        return pltpu.make_async_remote_copy(
            src_ref=src,
            dst_ref=cot_out.at[where],
            send_sem=ring_send.at[way, step - 1],
            recv_sem=ring_recv.at[way, step - 1],
            device_id={"tp": ring_next[way]},
            device_id_type=MESH,
        )

    def ring_landing(step, way):
        sign = 1 - 2 * way
        where = cot_rows(spot - sign * step, way, step == half_ring)
        return pltpu.make_async_remote_copy(
            src_ref=cot_out.at[where],
            dst_ref=cot_out.at[where],
            send_sem=ring_send.at[way, step - 1],
            recv_sem=ring_recv.at[way, step - 1],
            device_id={"tp": ring_next[way]},
            device_id_type=MESH,
        )

    def down_block(chip, which):
        block = chip * 2 + which
        if cols % 128:
            return down_out.at[block]
        return down_out.at[:, pl.ds(pl.multiple_of(block * cols, cols), cols)]

    def line_copy(step, way):
        sign = 1 - 2 * way
        where = down_block(z - sign * (step - 1), core)
        return pltpu.make_async_remote_copy(
            src_ref=down_ref if step == 1 else where,
            dst_ref=where,
            send_sem=line_send.at[way, step - 1],
            recv_sem=line_recv.at[way, step - 1],
            device_id={"fs": f + 2 * sign},
            device_id_type=MESH,
        )

    def line_landing(step, way):
        sign = 1 - 2 * way
        where = down_block(z - sign * step, core)
        return pltpu.make_async_remote_copy(
            src_ref=where,
            dst_ref=where,
            send_sem=line_send.at[way, step - 1],
            recv_sem=line_recv.at[way, step - 1],
            device_id={"fs": f + 2 * sign},
            device_id_type=MESH,
        )

    def pair_copy(step, way, which):
        sign = 1 - 2 * way
        where = down_block(z - sign * step, which)
        slot = step + way * (chips - 1)
        return pltpu.make_async_remote_copy(
            src_ref=down_ref if step == 0 else where,
            dst_ref=where,
            send_sem=pair_send.at[slot],
            recv_sem=pair_recv.at[slot],
            device_id={"fs": partner},
            device_id_type=MESH,
        )

    def has_landing(step, way):
        return z >= step if way == 0 else z + step < chips

    def has_copy(step, way):
        going = ahead if way == 0 else behind
        return going if step == 1 else jnp.logical_and(going, has_landing(step - 1, way))

    for way in range(2):
        ring_copy(1, way).start()

        @pl.when(has_copy(1, way))
        def _():
            line_copy(1, way).start()

    pair_copy(0, 0, core).start()
    own_cot = pltpu.make_async_copy(cot_ref, cot_out.at[pl.ds(q * rows, rows)], local_sem.at[0])
    own_down = pltpu.make_async_copy(down_ref, down_block(z, core), local_sem.at[1])
    own_cot.start()
    own_down.start()

    for step in range(1, max(chips - 1, half_ring) + 1):
        if step <= chips - 1:
            for way in range(2):

                @pl.when(has_landing(step, way))
                def _():
                    line_landing(step, way).wait_recv()
                    pair_copy(step, way, core).start()

                if step + 1 <= chips - 1:

                    @pl.when(has_copy(step + 1, way))
                    def _():
                        line_copy(step + 1, way).start()

        if step <= half_ring:
            for way in range(2):
                ring_landing(step, way).wait_recv()
                if step + 1 <= half_ring:
                    ring_copy(step + 1, way).start()

    own_cot.wait()
    own_down.wait()
    pair_copy(0, 0, 1 - core).wait_recv()
    pair_copy(0, 0, core).wait_send()
    for way in range(2):
        for step in range(1, half_ring + 1):
            ring_copy(step, way).wait_send()
        for step in range(1, chips):

            @pl.when(has_copy(step, way))
            def _():
                line_copy(step, way).wait_send()

            @pl.when(has_landing(step, way))
            def _():
                pair_copy(step, way, 1 - core).wait_recv()
                pair_copy(step, way, core).wait_send()


def gather_both(cotangent, down_proj):
    fs, tps = lax.axis_size("fs"), lax.axis_size("tp")
    chips = fs // 2
    rows, features = cotangent.shape
    channels, cols = down_proj.shape
    dma = pltpu.SemaphoreType.DMA
    down_shape = (fs, channels, cols) if cols % 128 else (channels, cols * fs)
    whole_cot, whole_down = pl.pallas_call(
        functools.partial(gather_kernel, chips, tps),
        out_shape=(
            jax.ShapeDtypeStruct((rows * tps, features), cotangent.dtype),
            jax.ShapeDtypeStruct(down_shape, down_proj.dtype),
        ),
        in_specs=[pl.BlockSpec(memory_space=pltpu.VMEM)] * 2,
        out_specs=[pl.BlockSpec(memory_space=pl.ANY)] * 2,
        scratch_shapes=[
            dma((2, tps // 2)),
            dma((2, tps // 2)),
            dma((2, chips - 1)),
            dma((2, chips - 1)),
            dma((2 * chips - 1,)),
            dma((2 * chips - 1,)),
            dma((2,)),
        ],
        compiler_params=pltpu.CompilerParams(collective_id=0, has_side_effects=True),
        name="gather_both",
    )(cotangent, down_proj)
    if cols % 128:
        whole_down = whole_down.transpose(1, 0, 2).reshape(channels, fs * cols)
    return whole_cot, whole_down


def small_kernel(fs, tps, mine_ref, sum_ref, all_ref, terms, total, sums, *sems):
    send_a, recv_a, send_b, recv_b = sems
    f, q = lax.axis_index("fs"), lax.axis_index("tp")
    barrier = pltpu.get_barrier_semaphore()
    for i in range(1, fs):
        pl.semaphore_signal(
            barrier, inc=1, device_id={"fs": (f + i) % fs}, device_id_type=MESH
        )
    for i in range(1, tps):
        pl.semaphore_signal(
            barrier, inc=1, device_id={"tp": (q + i) % tps}, device_id_type=MESH
        )
    pl.semaphore_wait(barrier, fs + tps - 2)

    def over_fs(i):
        return pltpu.make_async_remote_copy(
            src_ref=mine_ref,
            dst_ref=terms.at[f],
            send_sem=send_a.at[i],
            recv_sem=recv_a.at[i],
            device_id={"fs": (f + i) % fs},
            device_id_type=MESH,
        )

    def over_tp(i):
        return pltpu.make_async_remote_copy(
            src_ref=total,
            dst_ref=sums.at[q],
            send_sem=send_b.at[i],
            recv_sem=recv_b.at[i],
            device_id={"tp": (q + i) % tps},
            device_id_type=MESH,
        )

    def landing(buffer, slot, send, recv, i, device):
        return pltpu.make_async_remote_copy(
            src_ref=buffer.at[slot],
            dst_ref=buffer.at[slot],
            send_sem=send.at[i],
            recv_sem=recv.at[i],
            device_id=device,
            device_id_type=MESH,
        )

    for i in range(1, fs):
        over_fs(i).start()
    terms[f] = mine_ref[...]
    for i in range(1, fs):
        landing(terms, (f + fs - i) % fs, send_a, recv_a, i, {"fs": (f + i) % fs}).wait_recv()
    added = terms[0]
    for i in range(1, fs):
        added = added + terms[i]
    total[...] = added
    sum_ref[...] = added
    sums[q] = added
    for i in range(1, fs):
        over_fs(i).wait_send()
    for i in range(1, tps):
        over_tp(i).start()
    for i in range(1, tps):
        landing(sums, (q + tps - i) % tps, send_b, recv_b, i, {"tp": (q + i) % tps}).wait_recv()
    all_ref[...] = sums[...]
    for i in range(1, tps):
        over_tp(i).wait_send()


def small_sums(mine):
    fs, tps = lax.axis_size("fs"), lax.axis_size("tp")
    dma = pltpu.SemaphoreType.DMA
    shape = mine.shape
    return pl.pallas_call(
        functools.partial(small_kernel, fs, tps),
        out_shape=(
            jax.ShapeDtypeStruct(shape, jnp.float32),
            jax.ShapeDtypeStruct((tps,) + shape, jnp.float32),
        ),
        in_specs=[pl.BlockSpec(memory_space=pltpu.VMEM)],
        out_specs=[pl.BlockSpec(memory_space=pltpu.VMEM)] * 2,
        scratch_shapes=[
            pltpu.VMEM((fs,) + shape, jnp.float32),
            pltpu.VMEM(shape, jnp.float32),
            pltpu.VMEM((tps,) + shape, jnp.float32),
            dma((fs,)),
            dma((fs,)),
            dma((tps,)),
            dma((tps,)),
        ],
        compiler_params=pltpu.CompilerParams(collective_id=1, has_side_effects=True),
        name="small_sums",
    )(mine)


def from_behind(block, axis, distance):
    devices = range(lax.axis_size(axis))
    route = [(i - distance, i) for i in devices if i - distance in devices]
    return lax.ppermute(block, axis, route)


def staged_body(gate_pre, up_pre, gate_taps, up_taps, down_proj, cotangent):
    row_count = gate_pre.shape[0]
    channels = gate_pre.shape[1]
    tap_count = gate_taps.shape[0]
    reach = tap_count - 1
    channel_start = lax.axis_index("tp") * channels
    gate_taps_f = lax.dynamic_slice_in_dim(gate_taps, channel_start, channels, 1).astype(
        jnp.float32
    )
    up_taps_f = lax.dynamic_slice_in_dim(up_taps, channel_start, channels, 1).astype(jnp.float32)
    before = from_behind((gate_pre[row_count - reach :], up_pre[row_count - reach :]), "fs", 1)
    gate_padded = jnp.concatenate([before[0], gate_pre], axis=0).astype(jnp.float32)
    up_padded = jnp.concatenate([before[1], up_pre], axis=0).astype(jnp.float32)
    gate_conv = gate_taps_f[0] * gate_padded[0:row_count]
    up_conv = up_taps_f[0] * up_padded[0:row_count]
    for offset in range(1, tap_count):
        gate_conv = gate_conv + gate_taps_f[offset] * gate_padded[offset : offset + row_count]
        up_conv = up_conv + up_taps_f[offset] * up_padded[offset : offset + row_count]
    gate_sigmoid = jax.nn.sigmoid(gate_conv)
    gate_act = gate_conv * gate_sigmoid
    hidden = (gate_act * up_conv).astype(jnp.bfloat16)
    hidden = lax.optimization_barrier(hidden)
    whole_cot, whole_down = gather_both(cotangent, down_proj)
    grad_scale = 1.0 / math.sqrt(row_count * lax.axis_size("fs"))
    sum_type = jnp.bfloat16 if lax.axis_size("fs") <= 8 else jnp.float32
    terms = lax.dot_general(
        whole_cot, hidden, (((0,), (0,)), ((), ())), preferred_element_type=jnp.float32
    ).astype(sum_type)
    terms, whole_down = lax.optimization_barrier((terms, whole_down))
    own_rows = lax.psum_scatter(terms, "fs", scatter_dimension=0, tiled=True)
    own_rows = own_rows.astype(jnp.float32) * grad_scale
    hidden_grad = lax.dot_general(
        whole_cot,
        whole_down,
        (((1,), (1,)), ((), ())),
        preferred_element_type=jnp.float32,
    )
    gate_conv_grad = hidden_grad * up_conv * gate_sigmoid * (1.0 + gate_conv * (1.0 - gate_sigmoid))
    up_conv_grad = hidden_grad * gate_act
    following = from_behind((gate_conv_grad[0:reach], up_conv_grad[0:reach]), "fs", -1)
    gate_grad_pad = jnp.concatenate([gate_conv_grad, following[0]], axis=0)
    up_grad_pad = jnp.concatenate([up_conv_grad, following[1]], axis=0)
    gate_grad = gate_taps_f[0] * gate_grad_pad[reach : reach + row_count]
    up_grad = up_taps_f[0] * up_grad_pad[reach : reach + row_count]
    for offset in range(1, tap_count):
        lead = reach - offset
        gate_grad = gate_grad + gate_taps_f[offset] * gate_grad_pad[lead : lead + row_count]
        up_grad = up_grad + up_taps_f[offset] * up_grad_pad[lead : lead + row_count]
    gate_tap_terms = jnp.stack(
        [
            jnp.sum(gate_conv_grad * gate_padded[offset : offset + row_count], axis=0)
            for offset in range(tap_count)
        ]
    )
    up_tap_terms = jnp.stack(
        [
            jnp.sum(up_conv_grad * up_padded[offset : offset + row_count], axis=0)
            for offset in range(tap_count)
        ]
    )
    tap_terms = jnp.stack([gate_tap_terms, up_tap_terms])
    feature_count = whole_cot.shape[1]
    down_grad = own_rows.T
    partial_norms = jnp.sum(own_rows * own_rows, axis=0)
    tap_rows = tap_terms.reshape(2 * tap_count, channels)
    pad = -(2 * tap_count + 1) % 8
    mine = jnp.concatenate(
        [tap_rows, partial_norms[None], jnp.zeros((pad, channels), jnp.float32)], axis=0
    )
    summed, everywhere = small_sums(mine)
    row_norms = summed[2 * tap_count] / feature_count
    tap_grads = (
        everywhere[:, : 2 * tap_count].transpose(1, 0, 2).reshape(2, tap_count, -1) * grad_scale
    )
    return (
        gate_grad.astype(jnp.bfloat16),
        up_grad.astype(jnp.bfloat16),
        down_grad,
        row_norms,
        tap_grads,
    )


PIECES = 2
ROW_TILE = 128
SUB = 32
BLOCK = 64
LANES = 128
BF16_ROWS = 16


def less(a, b):
    return (b - a - 1 + 4096) // 4096


def whole_kernel(
    chips,
    tps,
    scale,
    gate_ref,
    up_ref,
    gtaps_ref,
    utaps_ref,
    down_ref,
    cot_ref,
    gate_out,
    up_out,
    down_out,
    norm_out,
    taps_out,
    gate_v,
    up_v,
    taps_v,
    a_v,
    b_v,
    hid_t,
    cot_v,
    down_v,
    pair_send,
    pair_recv,
    rs_recv,
    rs_send,
    dg_v,
    hg_v,
    edge_send,
    edge_recv,
    acc_v,
    tap_mine,
    tap_pair,
    tap_chip,
    tap_all,
    norm_all,
    *sems,
):
    (local, z_send, z_recv, pd_send, pd_recv, pt_send, pt_recv, c_send, c_recv) = sems[:9]
    (h_send, h_recv, e_send, e_recv, tp_send, tp_recv, tz_send, tz_recv) = sems[9:17]
    (ta_send, ta_recv, tb_send, tb_recv, n_send, n_recv) = sems[17:]
    f, q = lax.axis_index("fs"), lax.axis_index("tp")
    z, core = f // 2, f % 2
    fs = 2 * chips
    partner = z * 2 + 1 - core
    rows, features = cot_ref.shape
    channels, cols = down_ref.shape
    total_rows = rows * tps
    chip_cols = 2 * cols
    piece = channels // PIECES
    lane_tiles = channels // LANES
    half = z // (chips // 2)
    width = math.isqrt(tps)
    spot = snake(q, width)
    half_ring = tps // 2
    ring_next = (snake((spot + 1) % tps, width), snake((spot + tps - 1) % tps, width))
    f32, bf16 = jnp.float32, jnp.bfloat16

    def remote(src, dst, send, recv, device):
        return pltpu.make_async_remote_copy(
            src_ref=src,
            dst_ref=dst,
            send_sem=send,
            recv_sem=recv,
            device_id=device,
            device_id_type=MESH,
        )

    def down_piece(chip, which, s):
        col = pl.multiple_of(chip * chip_cols + which * cols, cols)
        return down_v.at[pl.ds(s * piece, piece), pl.ds(col, cols)]

    own_cot = pltpu.make_async_copy(
        cot_ref, cot_v.at[pl.ds(pl.multiple_of(q * rows, rows), rows)], local.at[0]
    )
    own_down = pltpu.make_async_copy(
        down_ref,
        down_v.at[:, pl.ds(pl.multiple_of(f * cols, cols), cols)],
        local.at[1],
    )
    load_gate = pltpu.make_async_copy(
        gate_ref, gate_v.at[pl.ds(BF16_ROWS, total_rows)], local.at[2]
    )
    load_up = pltpu.make_async_copy(up_ref, up_v.at[pl.ds(BF16_ROWS, total_rows)], local.at[3])
    own_down.start()
    own_cot.start()
    load_gate.start()
    load_up.start()

    barrier = pltpu.get_barrier_semaphore()
    for i in range(1, fs):
        pl.semaphore_signal(barrier, inc=1, device_id={"fs": (f + i) % fs}, device_id_type=MESH)
    for i in range(1, tps):
        pl.semaphore_signal(barrier, inc=1, device_id={"tp": (q + i) % tps}, device_id_type=MESH)
    pl.semaphore_wait(barrier, fs + tps - 2)

    def chip_at(position, way):
        return position + way * (chips - 1 - 2 * position)

    def z_copy(src, dst, way, p, s):
        return remote(
            src,
            dst,
            z_send.at[way, p, s],
            z_recv.at[way, p, s],
            {"fs": (f + 2 * (1 - 2 * way) + fs) % fs},
        )

    def pair_down(chip, which, s):
        where = down_piece(chip, which, s)
        return remote(where, where, pd_send.at[chip, s], pd_recv.at[chip, s], {"fs": partner})

    def halo_copy(i, src, dst):
        return remote(
            src.at[pl.ds(total_rows - BF16_ROWS, BF16_ROWS)],
            dst.at[pl.ds(0, BF16_ROWS)],
            h_send.at[i],
            h_recv.at[i],
            {"fs": (f + 1) % fs},
        )

    def chunk_chip(k):
        near = z + half * (chips - 1 - 2 * z)
        if k == chips - 1:
            position = near
        else:
            far = chips - 1 - near
            first = less(k, far)
            position = first * (chips - 1 - k) + (1 - first) * (k - far)
        return position + half * (chips - 1 - 2 * position)

    def cot_part(owner_spot, way, part, k):
        owner = snake((owner_spot + 2 * tps) % tps, width)
        col = pl.ds(pl.multiple_of(chunk_chip(k) * chip_cols, chip_cols), chip_cols)
        if part:
            start = owner * rows + way * (rows // 2)
            return cot_v.at[pl.ds(pl.multiple_of(start, rows // 2), rows // 2), col]
        return cot_v.at[pl.ds(pl.multiple_of(owner * rows, rows), rows), col]

    def ring_copy(k, step, way):
        sign = 1 - 2 * way
        where = cot_part(spot - sign * (step - 1), way, step == half_ring, k)
        return remote(
            where,
            where,
            c_send.at[k, way, step - 1],
            c_recv.at[k, way, step - 1],
            {"tp": ring_next[way]},
        )

    def ring_landing(k, step, way):
        sign = 1 - 2 * way
        where = cot_part(spot - sign * step, way, step == half_ring, k)
        return remote(
            where,
            where,
            c_send.at[k, way, step - 1],
            c_recv.at[k, way, step - 1],
            {"tp": ring_next[way]},
        )

    def ring_step(k, step):
        for way in range(2):
            ring_landing(k, step, way).wait_recv()
            if step < half_ring:
                ring_copy(k, step + 1, way).start()
        if step == 1:
            for ahead in range(1 + min(k, 1), 3):
                if k + ahead < chips:
                    for way in range(2):
                        ring_copy(k + ahead, 1, way).start()

    own_down.wait()

    @pl.when(f < fs - 1)
    def _():
        halo_copy(0, gate_ref, gate_v).start()
        halo_copy(1, up_ref, up_v).start()

    for s in range(PIECES):
        where = down_piece(z, core, s)

        @pl.when(z < chips - 1)
        def _():
            z_copy(where, where, 0, 0, s).start()

        @pl.when(z > 0)
        def _():
            z_copy(where, where, 1, 0, s).start()

    own_cot.wait()
    for way in range(2):
        ring_copy(0, 1, way).start()
    for s in range(PIECES):
        pair_down(z, core, s).start()

    tap_col = pl.multiple_of(q * channels, LANES)
    taps_v[0, 0:3, :] = gtaps_ref[:, pl.ds(tap_col, channels)].astype(f32)
    taps_v[1, 0:3, :] = utaps_ref[:, pl.ds(tap_col, channels)].astype(f32)

    def hidden_tile(tile, lane_tile):
        lane = pl.ds(pl.multiple_of(lane_tile * LANES, LANES), LANES)
        gt = [taps_v[0, k : k + 1, lane] for k in range(3)]
        ut = [taps_v[1, k : k + 1, lane] for k in range(3)]
        parts = []
        for i in range(ROW_TILE // SUB):
            start = pl.multiple_of(tile * ROW_TILE + i * SUB, SUB)
            window = pl.ds(start, SUB + BF16_ROWS)
            g = gate_v[window, lane].astype(f32)
            u = up_v[window, lane].astype(f32)
            g_conv = (
                gt[0] * pltpu.roll(g, 2, 0)[BF16_ROWS:]
                + gt[1] * pltpu.roll(g, 1, 0)[BF16_ROWS:]
                + gt[2] * g[BF16_ROWS:]
            )
            u_conv = (
                ut[0] * pltpu.roll(u, 2, 0)[BF16_ROWS:]
                + ut[1] * pltpu.roll(u, 1, 0)[BF16_ROWS:]
                + ut[2] * u[BF16_ROWS:]
            )
            sig = 0.5 * jnp.tanh(0.5 * g_conv) + 0.5
            act = g_conv * sig
            out = pl.ds(start, SUB)
            a_v[out, lane] = u_conv * (sig + act * (1.0 - sig))
            b_v[out, lane] = act
            parts.append((act * u_conv).astype(bf16))
        tile_t = jnp.concatenate(parts, axis=0).T
        hid_t[lane, pl.ds(pl.multiple_of(tile * ROW_TILE, ROW_TILE), ROW_TILE)] = tile_t

    def hidden_tiles(first, count):
        def step(i, carry):
            hidden_tile(first + i // lane_tiles, i % lane_tiles)
            return carry

        lax.fori_loop(0, count * lane_tiles, step, 0)

    tiles = total_rows // ROW_TILE
    load_gate.wait()
    load_up.wait()
    hidden_tiles(tiles // 2, tiles - tiles // 2)
    ring_step(0, 1)
    hidden_tiles(1, tiles // 2 - 1)

    @pl.when(f > 0)
    def _():
        halo_copy(0, gate_ref, gate_v).wait_recv()
        halo_copy(1, up_ref, up_v).wait_recv()

    @pl.when(f == 0)
    def _():
        gate_v[0:BF16_ROWS, :] = jnp.zeros((BF16_ROWS, channels), bf16)
        up_v[0:BF16_ROWS, :] = jnp.zeros((BF16_ROWS, channels), bf16)

    hidden_tiles(0, 1)

    def terms(s, chip, which):
        col = pl.multiple_of(chip * chip_cols + which * cols, cols)
        return jnp.dot(
            hid_t[pl.ds(pl.multiple_of(s * piece, BF16_ROWS), piece), :],
            cot_v[:, pl.ds(col, cols)],
            preferred_element_type=f32,
        )

    def pair_terms_copy(chip):
        return remote(
            pair_send.at[chip],
            pair_recv.at[chip],
            pt_send.at[chip],
            pt_recv.at[chip],
            {"fs": partner},
        )

    def pair_terms(k):
        chip = chunk_chip(k)

        def step(s, carry):
            here = pl.ds(pl.multiple_of(s * piece, BF16_ROWS), piece)
            pair_send[chip, here, :] = terms(s, chip, 1 - core).astype(bf16)
            return carry

        lax.fori_loop(0, PIECES, step, 0)
        pair_terms_copy(chip).start()

    def pair_terms_wait(k):
        pair_terms_copy(chunk_chip(k)).wait_recv()

    def send_sum(position, way, p, s, first):
        chip = chip_at(chips - 1 + position - p, way)
        here = pl.ds(s * piece, piece)
        value = terms(s, chip, core) + pair_recv[chip, here, :].astype(f32)
        if not first:
            earlier = rs_recv[way, chip, here, :].astype(f32)
            value = value + jnp.where(position > 0, earlier, 0.0)
        rs_send[chip, here, :] = value.astype(bf16)
        z_copy(rs_send.at[chip, here], rs_recv.at[way, chip, here], way, p + 1, s).start()

    def both_ways(body):
        def step(d, carry):
            way = (half + d) % 2
            body(way, z + way * (chips - 1 - 2 * z))
            return carry

        lax.fori_loop(0, 2, step, 0)

    def first_sums():
        def body(way, position):
            @pl.when(position == 0)
            def _():
                for s in range(PIECES):
                    send_sum(position, way, 0, s, True)

        both_ways(body)

    def slot(p, s):
        here = pl.ds(s * piece, piece)

        def body(way, position):
            @pl.when(position > p)
            def _():
                chip = chip_at(position - 1 - p, way)
                where = down_piece(chip, core, s)
                z_copy(where, where, way, p, s).wait_recv()
                if p + 1 < chips:

                    @pl.when(position < chips - 1)
                    def _():
                        z_copy(where, where, way, p + 1, s).start()

                pair_down(chip, core, s).start()

            if p > 0:

                @pl.when(jnp.logical_and(position > 0, position <= p))
                def _():
                    chip = chip_at(chips - 1 + position - p, way)
                    where = rs_recv.at[way, chip, here]
                    z_copy(where, where, way, p, s).wait_recv()

                if p + 1 < chips:

                    @pl.when(position <= p)
                    def _():
                        send_sum(position, way, p, s, False)

        both_ways(body)

    def pair_down_wait(chip):
        for s in range(PIECES):
            pair_down(chip, 1 - core, s).wait_recv()

    last_chip = (1 - half) * (chips - 1)

    def hidden_grad(first_chip, count, add):
        depth = count * chip_cols
        col = pl.ds(pl.multiple_of(first_chip * chip_cols, chip_cols), depth)

        def one(start, size):
            lane = pl.ds(start, size)
            value = lax.dot_general(
                cot_v[:, col],
                down_v[lane, col],
                (((1,), (1,)), ((), ())),
                preferred_element_type=f32,
            )
            if add:
                value = value + hg_v[0:total_rows, lane]
            hg_v[0:total_rows, lane] = value

        wide = 2 * LANES

        def step(n, carry):
            one(pl.multiple_of(n * wide, wide), wide)
            return carry

        lax.fori_loop(0, channels // wide, step, 0)
        if channels % wide:
            one(channels - channels % wide, channels % wide)

    slot(0, 0)
    for step in range(2, half_ring + 1):
        ring_step(0, step)
    pair_terms(0)
    pair_terms_wait(0)
    first_sums()
    for s in range(1, PIECES):
        slot(0, s)
    ring_step(1, 1)
    for p in range(1, chips - 1):
        ring_step(p + 1, 1)
        for step in range(2, half_ring + 1):
            ring_step(p, step)
        pair_terms(p)
        pair_terms_wait(p)
        if p < chips - 2:
            for s in range(PIECES):
                slot(p, s)
    for step in range(2, half_ring + 1):
        ring_step(chips - 1, step)
    pair_terms(chips - 1)
    slot(chips - 2, 0)
    for i in range(chips - 1):
        pair_down_wait(half + i)
    hidden_grad(half, chips - 1, False)
    pair_terms_wait(chips - 1)
    for s in range(1, PIECES):
        slot(chips - 2, s)

    def own_terms(s, carry):
        here = pl.ds(pl.multiple_of(s * piece, BF16_ROWS), piece)
        dg_v[here, :] = terms(s, z, core) + pair_recv[z, here, :].astype(f32)
        return carry

    lax.fori_loop(0, PIECES, own_terms, 0)
    pair_down_wait(last_chip)
    hidden_grad(last_chip, 1, True)

    edge = 8
    row_index = lax.broadcasted_iota(jnp.int32, (edge, channels), 0)
    top = pl.ds(0, edge)
    edge_send[...] = jnp.where(
        row_index < 2,
        hg_v[top, :] * a_v[top, :],
        pltpu.roll(hg_v[top, :] * b_v[top, :], 2, 0),
    )
    edge_copy = remote(
        edge_send, edge_recv, e_send.at[0], e_recv.at[0], {"fs": (f + fs - 1) % fs}
    )

    @pl.when(f > 0)
    def _():
        edge_copy.start()

    def grads(start, lane, sums):
        window = pl.ds(start, BLOCK + edge)
        here = pl.ds(pl.multiple_of(start + BF16_ROWS, BF16_ROWS), BLOCK)
        hg = hg_v[window, lane]
        new = []
        for b, (factor, pre) in enumerate(((a_v, gate_v), (b_v, up_v))):
            g = hg * factor[window, lane]
            g0 = g[0:BLOCK]
            g1 = pltpu.roll(g, BLOCK + edge - 1, 0)[0:BLOCK]
            g2 = pltpu.roll(g, BLOCK + edge - 2, 0)[0:BLOCK]
            x = pre[here, lane].astype(f32)
            for i, shifted in enumerate((g2, g1, g0)):
                product = (shifted * x).reshape(BLOCK // 8, 8, LANES)
                new.append(sums[3 * b + i] + jnp.sum(product, axis=0))
            t = [taps_v[b, k : k + 1, lane] for k in range(3)]
            pre[here, lane] = (t[0] * g2 + t[1] * g1 + t[2] * g0).astype(bf16)
        return tuple(new)

    blocks = total_rows // BLOCK

    def grad_lanes(lane_tile, carry):
        lane = pl.ds(pl.multiple_of(lane_tile * LANES, LANES), LANES)

        def step(i, sums):
            return grads(pl.multiple_of(i * BLOCK, BLOCK), lane, sums)

        zero = jnp.zeros((8, LANES), f32)
        sums = lax.fori_loop(0, blocks - 1, step, (zero,) * 6)
        for i in range(6):
            acc_v[i, :, lane] = sums[i]
        return carry

    def grad_last(lane_tile, carry):
        lane = pl.ds(pl.multiple_of(lane_tile * LANES, LANES), LANES)
        sums = grads((blocks - 1) * BLOCK, lane, tuple(acc_v[i, :, lane] for i in range(6)))
        for b in range(2):
            for k in range(3):
                tap_mine[b, k : k + 1, lane] = jnp.sum(sums[3 * b + k], axis=0, keepdims=True)
        return carry

    lax.fori_loop(0, lane_tiles // 2, grad_lanes, 0)
    lax.fori_loop(lane_tiles // 2, lane_tiles, grad_lanes, 0)

    @pl.when(f < fs - 1)
    def _():
        edge_copy.wait_recv()

    @pl.when(f == fs - 1)
    def _():
        edge_recv[...] = jnp.zeros((edge, channels), f32)

    bottom = pl.ds(total_rows, edge)
    hg_v[bottom, :] = jnp.ones((edge, channels), f32)
    a_v[bottom, :] = edge_recv[...]
    b_v[bottom, :] = pltpu.roll(edge_recv[...], edge - 2, 0)
    tap_mine[...] = jnp.zeros(tap_mine.shape, f32)
    lax.fori_loop(0, lane_tiles, grad_last, 0)
    store_gate = pltpu.make_async_copy(
        gate_v.at[pl.ds(BF16_ROWS, total_rows)], gate_out, local.at[4]
    )
    store_up = pltpu.make_async_copy(up_v.at[pl.ds(BF16_ROWS, total_rows)], up_out, local.at[5])
    store_gate.start()
    store_up.start()

    tap_pair_copy = remote(
        tap_mine.at[1 - core], tap_pair, tp_send.at[0], tp_recv.at[0], {"fs": partner}
    )
    tap_pair_copy.start()

    def tap_chip_copy(i, sender):
        return remote(
            tap_chip.at[sender],
            tap_chip.at[sender],
            tz_send.at[i],
            tz_recv.at[sender],
            {"fs": ((z + i) % chips) * 2 + core},
        )

    tap_pair_copy.wait_recv()
    tap_chip[z] = tap_mine[core] + tap_pair[...]
    for i in range(1, chips):
        tap_chip_copy(i, z).start()
    for i in range(1, chips):
        tap_chip_copy(i, (z + i) % chips).wait_recv()
    total = tap_chip[0]
    for i in range(1, chips):
        total = total + tap_chip[i]
    tap_all[core, q] = total * scale

    def tap_all_copy(i, sender):
        return remote(
            tap_all.at[core, sender],
            tap_all.at[core, sender],
            ta_send.at[i],
            ta_recv.at[sender],
            {"tp": (q + i) % tps},
        )

    for i in range(1, tps):
        tap_all_copy(i, q).start()

    for s in range(PIECES):
        slot(chips - 1, s)

    ones = jnp.ones((8, cols), bf16)

    def finish(s, carry):
        here = pl.ds(pl.multiple_of(s * piece, BF16_ROWS), piece)
        value = dg_v[here, :]
        value = value + jnp.where(z > 0, rs_recv[0, z, here, :].astype(f32), 0.0)
        value = value + jnp.where(z < chips - 1, rs_recv[1, z, here, :].astype(f32), 0.0)
        dg_v[here, :] = value * scale
        return carry

    lax.fori_loop(0, PIECES, finish, 0)
    store_down = pltpu.make_async_copy(dg_v, down_out, local.at[6])
    store_down.start()
    contract = (((1,), (1,)), ((), ()))
    value = dg_v[...]
    square = value * value
    high = square.astype(bf16)
    low = (square - high.astype(f32)).astype(bf16)
    norm = lax.dot_general(ones, high, contract, preferred_element_type=f32)
    norm = norm + lax.dot_general(ones, low, contract, preferred_element_type=f32)
    norm_all[f] = norm[0:1]

    def norm_copy(i, sender):
        return remote(
            norm_all.at[sender],
            norm_all.at[sender],
            n_send.at[i],
            n_recv.at[sender],
            {"fs": (f + i) % fs},
        )

    for i in range(1, fs):
        norm_copy(i, f).start()
    for i in range(1, tps):
        tap_all_copy(i, (q + i) % tps).wait_recv()

    def tap_both_copy(which):
        return remote(
            tap_all.at[which], tap_all.at[which], tb_send.at[0], tb_recv.at[0], {"fs": partner}
        )

    tap_both_copy(core).start()
    for i in range(1, fs):
        norm_copy(i, (f + i) % fs).wait_recv()
    total = norm_all[0]
    for i in range(1, fs):
        total = total + norm_all[i]
    norm_out[...] = total * (1.0 / features)
    tap_both_copy(1 - core).wait_recv()
    for b in range(2):
        for i in range(tps):
            taps_out[b, :, i * channels : (i + 1) * channels] = tap_all[b, i, 0:3, :]

    store_gate.wait()
    store_up.wait()
    store_down.wait()

    @pl.when(f < fs - 1)
    def _():
        halo_copy(0, gate_ref, gate_v).wait_send()
        halo_copy(1, up_ref, up_v).wait_send()

    @pl.when(f > 0)
    def _():
        edge_copy.wait_send()

    for k in range(chips):
        for way in range(2):
            for step in range(1, half_ring + 1):
                ring_copy(k, step, way).wait_send()
        pair_terms_copy(k).wait_send()
        for s in range(PIECES):
            pair_down(k, core, s).wait_send()

    for p in range(chips):
        for s in range(PIECES):
            where = rs_send.at[0, pl.ds(s * piece, piece)]

            @pl.when(z < chips - 1)
            def _():
                z_copy(where, where, 0, p, s).wait_send()

            @pl.when(z > 0)
            def _():
                z_copy(where, where, 1, p, s).wait_send()

    tap_pair_copy.wait_send()
    tap_both_copy(core).wait_send()
    for i in range(1, chips):
        tap_chip_copy(i, z).wait_send()
    for i in range(1, tps):
        tap_all_copy(i, q).wait_send()
    for i in range(1, fs):
        norm_copy(i, f).wait_send()


def whole_body(gate_pre, up_pre, gate_taps, up_taps, down_proj, cotangent):
    fs, tps = lax.axis_size("fs"), lax.axis_size("tp")
    chips = fs // 2
    rows, features = cotangent.shape
    channels, cols = down_proj.shape
    total = rows * tps
    f32, bf16 = jnp.float32, jnp.bfloat16
    dma = pltpu.SemaphoreType.DMA
    scale = 1.0 / math.sqrt(total * fs)
    ring = (chips, 2, tps // 2)
    gate_grad, up_grad, down_grad, norms, taps = pl.pallas_call(
        functools.partial(whole_kernel, chips, tps, scale),
        out_shape=(
            jax.ShapeDtypeStruct((total, channels), bf16),
            jax.ShapeDtypeStruct((total, channels), bf16),
            jax.ShapeDtypeStruct((channels, cols), f32),
            jax.ShapeDtypeStruct((1, channels), f32),
            jax.ShapeDtypeStruct((2, 3, channels * tps), f32),
        ),
        in_specs=[
            pl.BlockSpec(memory_space=pl.ANY),
            pl.BlockSpec(memory_space=pl.ANY),
            pl.BlockSpec(memory_space=pltpu.VMEM),
            pl.BlockSpec(memory_space=pltpu.VMEM),
            pl.BlockSpec(memory_space=pl.ANY),
            pl.BlockSpec(memory_space=pl.ANY),
        ],
        out_specs=[
            pl.BlockSpec(memory_space=pl.ANY),
            pl.BlockSpec(memory_space=pl.ANY),
            pl.BlockSpec(memory_space=pl.ANY),
            pl.BlockSpec(memory_space=pltpu.VMEM),
            pl.BlockSpec(memory_space=pltpu.VMEM),
        ],
        scratch_shapes=[
            pltpu.VMEM((total + BF16_ROWS, channels), bf16),
            pltpu.VMEM((total + BF16_ROWS, channels), bf16),
            pltpu.VMEM((2, 4, channels), f32),
            pltpu.VMEM((total + 8, channels), f32),
            pltpu.VMEM((total + 8, channels), f32),
            pltpu.VMEM((channels, total), bf16),
            pltpu.VMEM((total, features), bf16),
            pltpu.VMEM((channels, features), bf16),
            pltpu.VMEM((chips, channels, cols), bf16),
            pltpu.VMEM((chips, channels, cols), bf16),
            pltpu.VMEM((2, chips, channels, cols), bf16),
            pltpu.VMEM((chips, channels, cols), bf16),
            pltpu.VMEM((channels, cols), f32),
            pltpu.VMEM((total + 8, channels), f32),
            pltpu.VMEM((8, channels), f32),
            pltpu.VMEM((8, channels), f32),
            pltpu.VMEM((6, 8, channels), f32),
            pltpu.VMEM((2, 4, channels), f32),
            pltpu.VMEM((4, channels), f32),
            pltpu.VMEM((chips, 4, channels), f32),
            pltpu.VMEM((2, tps, 4, channels), f32),
            pltpu.VMEM((fs, 1, channels), f32),
            dma((7,)),
            dma((2, chips, PIECES)),
            dma((2, chips, PIECES)),
            dma((chips, PIECES)),
            dma((chips, PIECES)),
            dma((chips,)),
            dma((chips,)),
            dma(ring),
            dma(ring),
            dma((2,)),
            dma((2,)),
            dma((1,)),
            dma((1,)),
            dma((1,)),
            dma((1,)),
            dma((chips,)),
            dma((chips,)),
            dma((tps,)),
            dma((tps,)),
            dma((1,)),
            dma((1,)),
            dma((fs,)),
            dma((fs,)),
        ],
        compiler_params=pltpu.CompilerParams(
            collective_id=2, has_side_effects=True, vmem_limit_bytes=VMEM_BYTES
        ),
        name="whole_layer",
    )(gate_pre, up_pre, gate_taps, up_taps, down_proj, cotangent)
    return gate_grad, up_grad, down_grad, norms.reshape(channels), taps


VMEM_BYTES = 67_043_328


def fits_whole(gate_pre, gate_taps, down_proj, cotangent):
    fs, tps = lax.axis_size("fs"), lax.axis_size("tp")
    chips = fs // 2
    channels, cols = down_proj.shape
    rows, features = cotangent.shape
    total = rows * tps
    tiled = channels % (LANES * PIECES // 2) == 0 and cols % (2 * LANES) == 0
    tiled = tiled and channels % (BF16_ROWS * PIECES) == 0 and total % ROW_TILE == 0
    tiled = tiled and rows % (2 * BF16_ROWS) == 0 and gate_taps.shape[0] == 3
    tiled = tiled and fs % 2 == 0 and chips % 2 == 0 and chips >= 4 and tps >= 4
    held = 2 * total * channels * (2 + 4) + total * channels * (2 + 4)
    held += (total + channels) * features * 2 + channels * cols * (5 * chips * 2 + 4)
    return tiled and held < VMEM_BYTES * 7 // 8


def body(gate_pre, up_pre, gate_taps, up_taps, down_proj, cotangent):
    args = (gate_pre, up_pre, gate_taps, up_taps, down_proj, cotangent)
    if fits_whole(gate_pre, gate_taps, down_proj, cotangent):
        return whole_body(*args)
    return staged_body(*args)


def solution(mesh):
    placed = (P("fs", "tp"), P("fs", "tp"), P(), P(), P("tp", "fs"), P(("fs", "tp"), None))
    return jax.shard_map(
        body,
        mesh=mesh,
        in_specs=placed,
        out_specs=(P("fs", "tp"), P("fs", "tp"), P("tp", "fs"), P("tp"), P()),
        check_vma=False,
    )
```

```python
import functools
import math

import jax
import jax.numpy as jnp
from jax import lax
from jax.experimental import pallas as pl
from jax.experimental.pallas import tpu as pltpu
from jax.sharding import PartitionSpec as P

MESH = pl.DeviceIdType.MESH


def snake(position, width):
    row, column = position // width, position % width
    return row * width + column + (row % 2) * (width - 1 - 2 * column)


def gather_kernel(chips, tps, cot_ref, down_ref, cot_out, down_out, *sems):
    (ring_send, ring_recv, line_send, line_recv, pair_send, pair_recv, local_sem) = sems
    f, q = lax.axis_index("fs"), lax.axis_index("tp")
    z, core = f // 2, f % 2
    width = math.isqrt(tps)
    spot = snake(q, width)
    half_ring = tps // 2
    ring_next = (snake((spot + 1) % tps, width), snake((spot + tps - 1) % tps, width))
    rows = cot_ref.shape[0]
    cols = down_ref.shape[1]
    partner = z * 2 + 1 - core
    behind, ahead = z > 0, z < chips - 1

    barrier = pltpu.get_barrier_semaphore()
    for device in ({"tp": ring_next[0]}, {"tp": ring_next[1]}, {"fs": partner}):
        pl.semaphore_signal(barrier, inc=1, device_id=device, device_id_type=MESH)

    @pl.when(behind)
    def _():
        pl.semaphore_signal(barrier, inc=1, device_id={"fs": f - 2}, device_id_type=MESH)

    @pl.when(ahead)
    def _():
        pl.semaphore_signal(barrier, inc=1, device_id={"fs": f + 2}, device_id_type=MESH)

    pl.semaphore_wait(barrier, 4 + (z + chips - 1) // chips - (z + 1) // chips)

    def cot_rows(owner_spot, way, part):
        owner = snake((owner_spot + 2 * tps) % tps, width)
        if part:
            return pl.ds(owner * rows + way * (rows // 2), rows // 2)
        return pl.ds(owner * rows, rows)

    def ring_copy(step, way):
        sign = 1 - 2 * way
        part = step == half_ring
        where = cot_rows(spot - sign * (step - 1), way, part)
        if step == 1:
            src = cot_ref.at[pl.ds(way * (rows // 2), rows // 2)] if part else cot_ref
        else:
            src = cot_out.at[where]
        return pltpu.make_async_remote_copy(
            src_ref=src,
            dst_ref=cot_out.at[where],
            send_sem=ring_send.at[way, step - 1],
            recv_sem=ring_recv.at[way, step - 1],
            device_id={"tp": ring_next[way]},
            device_id_type=MESH,
        )

    def ring_landing(step, way):
        sign = 1 - 2 * way
        where = cot_rows(spot - sign * step, way, step == half_ring)
        return pltpu.make_async_remote_copy(
            src_ref=cot_out.at[where],
            dst_ref=cot_out.at[where],
            send_sem=ring_send.at[way, step - 1],
            recv_sem=ring_recv.at[way, step - 1],
            device_id={"tp": ring_next[way]},
            device_id_type=MESH,
        )

    def down_block(chip, which):
        block = chip * 2 + which
        if cols % 128:
            return down_out.at[block]
        return down_out.at[:, pl.ds(pl.multiple_of(block * cols, cols), cols)]

    def line_copy(step, way):
        sign = 1 - 2 * way
        where = down_block(z - sign * (step - 1), core)
        return pltpu.make_async_remote_copy(
            src_ref=down_ref if step == 1 else where,
            dst_ref=where,
            send_sem=line_send.at[way, step - 1],
            recv_sem=line_recv.at[way, step - 1],
            device_id={"fs": f + 2 * sign},
            device_id_type=MESH,
        )

    def line_landing(step, way):
        sign = 1 - 2 * way
        where = down_block(z - sign * step, core)
        return pltpu.make_async_remote_copy(
            src_ref=where,
            dst_ref=where,
            send_sem=line_send.at[way, step - 1],
            recv_sem=line_recv.at[way, step - 1],
            device_id={"fs": f + 2 * sign},
            device_id_type=MESH,
        )

    def pair_copy(step, way, which):
        sign = 1 - 2 * way
        where = down_block(z - sign * step, which)
        slot = step + way * (chips - 1)
        return pltpu.make_async_remote_copy(
            src_ref=down_ref if step == 0 else where,
            dst_ref=where,
            send_sem=pair_send.at[slot],
            recv_sem=pair_recv.at[slot],
            device_id={"fs": partner},
            device_id_type=MESH,
        )

    def has_landing(step, way):
        return z >= step if way == 0 else z + step < chips

    def has_copy(step, way):
        going = ahead if way == 0 else behind
        return going if step == 1 else jnp.logical_and(going, has_landing(step - 1, way))

    for way in range(2):
        ring_copy(1, way).start()

        @pl.when(has_copy(1, way))
        def _():
            line_copy(1, way).start()

    pair_copy(0, 0, core).start()
    own_cot = pltpu.make_async_copy(cot_ref, cot_out.at[pl.ds(q * rows, rows)], local_sem.at[0])
    own_down = pltpu.make_async_copy(down_ref, down_block(z, core), local_sem.at[1])
    own_cot.start()
    own_down.start()

    for step in range(1, max(chips - 1, half_ring) + 1):
        if step <= chips - 1:
            for way in range(2):

                @pl.when(has_landing(step, way))
                def _():
                    line_landing(step, way).wait_recv()
                    pair_copy(step, way, core).start()

                if step + 1 <= chips - 1:

                    @pl.when(has_copy(step + 1, way))
                    def _():
                        line_copy(step + 1, way).start()

        if step <= half_ring:
            for way in range(2):
                ring_landing(step, way).wait_recv()
                if step + 1 <= half_ring:
                    ring_copy(step + 1, way).start()

    own_cot.wait()
    own_down.wait()
    pair_copy(0, 0, 1 - core).wait_recv()
    pair_copy(0, 0, core).wait_send()
    for way in range(2):
        for step in range(1, half_ring + 1):
            ring_copy(step, way).wait_send()
        for step in range(1, chips):

            @pl.when(has_copy(step, way))
            def _():
                line_copy(step, way).wait_send()

            @pl.when(has_landing(step, way))
            def _():
                pair_copy(step, way, 1 - core).wait_recv()
                pair_copy(step, way, core).wait_send()


def gather_both(cotangent, down_proj):
    fs, tps = lax.axis_size("fs"), lax.axis_size("tp")
    chips = fs // 2
    rows, features = cotangent.shape
    channels, cols = down_proj.shape
    dma = pltpu.SemaphoreType.DMA
    down_shape = (fs, channels, cols) if cols % 128 else (channels, cols * fs)
    whole_cot, whole_down = pl.pallas_call(
        functools.partial(gather_kernel, chips, tps),
        out_shape=(
            jax.ShapeDtypeStruct((rows * tps, features), cotangent.dtype),
            jax.ShapeDtypeStruct(down_shape, down_proj.dtype),
        ),
        in_specs=[pl.BlockSpec(memory_space=pltpu.VMEM)] * 2,
        out_specs=[pl.BlockSpec(memory_space=pl.ANY)] * 2,
        scratch_shapes=[
            dma((2, tps // 2)),
            dma((2, tps // 2)),
            dma((2, chips - 1)),
            dma((2, chips - 1)),
            dma((2 * chips - 1,)),
            dma((2 * chips - 1,)),
            dma((2,)),
        ],
        compiler_params=pltpu.CompilerParams(collective_id=0, has_side_effects=True),
        name="gather_both",
    )(cotangent, down_proj)
    if cols % 128:
        whole_down = whole_down.transpose(1, 0, 2).reshape(channels, fs * cols)
    return whole_cot, whole_down


def small_kernel(fs, tps, mine_ref, sum_ref, all_ref, terms, total, sums, *sems):
    send_a, recv_a, send_b, recv_b = sems
    f, q = lax.axis_index("fs"), lax.axis_index("tp")
    barrier = pltpu.get_barrier_semaphore()
    for i in range(1, fs):
        pl.semaphore_signal(
            barrier, inc=1, device_id={"fs": (f + i) % fs}, device_id_type=MESH
        )
    for i in range(1, tps):
        pl.semaphore_signal(
            barrier, inc=1, device_id={"tp": (q + i) % tps}, device_id_type=MESH
        )
    pl.semaphore_wait(barrier, fs + tps - 2)

    def over_fs(i):
        return pltpu.make_async_remote_copy(
            src_ref=mine_ref,
            dst_ref=terms.at[f],
            send_sem=send_a.at[i],
            recv_sem=recv_a.at[i],
            device_id={"fs": (f + i) % fs},
            device_id_type=MESH,
        )

    def over_tp(i):
        return pltpu.make_async_remote_copy(
            src_ref=total,
            dst_ref=sums.at[q],
            send_sem=send_b.at[i],
            recv_sem=recv_b.at[i],
            device_id={"tp": (q + i) % tps},
            device_id_type=MESH,
        )

    def landing(buffer, slot, send, recv, i, device):
        return pltpu.make_async_remote_copy(
            src_ref=buffer.at[slot],
            dst_ref=buffer.at[slot],
            send_sem=send.at[i],
            recv_sem=recv.at[i],
            device_id=device,
            device_id_type=MESH,
        )

    for i in range(1, fs):
        over_fs(i).start()
    terms[f] = mine_ref[...]
    for i in range(1, fs):
        landing(terms, (f + fs - i) % fs, send_a, recv_a, i, {"fs": (f + i) % fs}).wait_recv()
    added = terms[0]
    for i in range(1, fs):
        added = added + terms[i]
    total[...] = added
    sum_ref[...] = added
    sums[q] = added
    for i in range(1, fs):
        over_fs(i).wait_send()
    for i in range(1, tps):
        over_tp(i).start()
    for i in range(1, tps):
        landing(sums, (q + tps - i) % tps, send_b, recv_b, i, {"tp": (q + i) % tps}).wait_recv()
    all_ref[...] = sums[...]
    for i in range(1, tps):
        over_tp(i).wait_send()


def small_sums(mine):
    fs, tps = lax.axis_size("fs"), lax.axis_size("tp")
    dma = pltpu.SemaphoreType.DMA
    shape = mine.shape
    return pl.pallas_call(
        functools.partial(small_kernel, fs, tps),
        out_shape=(
            jax.ShapeDtypeStruct(shape, jnp.float32),
            jax.ShapeDtypeStruct((tps,) + shape, jnp.float32),
        ),
        in_specs=[pl.BlockSpec(memory_space=pltpu.VMEM)],
        out_specs=[pl.BlockSpec(memory_space=pltpu.VMEM)] * 2,
        scratch_shapes=[
            pltpu.VMEM((fs,) + shape, jnp.float32),
            pltpu.VMEM(shape, jnp.float32),
            pltpu.VMEM((tps,) + shape, jnp.float32),
            dma((fs,)),
            dma((fs,)),
            dma((tps,)),
            dma((tps,)),
        ],
        compiler_params=pltpu.CompilerParams(collective_id=1, has_side_effects=True),
        name="small_sums",
    )(mine)


def from_behind(block, axis, distance):
    devices = range(lax.axis_size(axis))
    route = [(i - distance, i) for i in devices if i - distance in devices]
    return lax.ppermute(block, axis, route)


def staged_body(gate_pre, up_pre, gate_taps, up_taps, down_proj, cotangent):
    row_count = gate_pre.shape[0]
    channels = gate_pre.shape[1]
    tap_count = gate_taps.shape[0]
    reach = tap_count - 1
    channel_start = lax.axis_index("tp") * channels
    gate_taps_f = lax.dynamic_slice_in_dim(gate_taps, channel_start, channels, 1).astype(
        jnp.float32
    )
    up_taps_f = lax.dynamic_slice_in_dim(up_taps, channel_start, channels, 1).astype(jnp.float32)
    before = from_behind((gate_pre[row_count - reach :], up_pre[row_count - reach :]), "fs", 1)
    gate_padded = jnp.concatenate([before[0], gate_pre], axis=0).astype(jnp.float32)
    up_padded = jnp.concatenate([before[1], up_pre], axis=0).astype(jnp.float32)
    gate_conv = gate_taps_f[0] * gate_padded[0:row_count]
    up_conv = up_taps_f[0] * up_padded[0:row_count]
    for offset in range(1, tap_count):
        gate_conv = gate_conv + gate_taps_f[offset] * gate_padded[offset : offset + row_count]
        up_conv = up_conv + up_taps_f[offset] * up_padded[offset : offset + row_count]
    gate_sigmoid = jax.nn.sigmoid(gate_conv)
    gate_act = gate_conv * gate_sigmoid
    hidden = (gate_act * up_conv).astype(jnp.bfloat16)
    hidden = lax.optimization_barrier(hidden)
    whole_cot, whole_down = gather_both(cotangent, down_proj)
    grad_scale = 1.0 / math.sqrt(row_count * lax.axis_size("fs"))
    sum_type = jnp.bfloat16 if lax.axis_size("fs") <= 8 else jnp.float32
    terms = lax.dot_general(
        whole_cot, hidden, (((0,), (0,)), ((), ())), preferred_element_type=jnp.float32
    ).astype(sum_type)
    terms, whole_down = lax.optimization_barrier((terms, whole_down))
    own_rows = lax.psum_scatter(terms, "fs", scatter_dimension=0, tiled=True)
    own_rows = own_rows.astype(jnp.float32) * grad_scale
    hidden_grad = lax.dot_general(
        whole_cot,
        whole_down,
        (((1,), (1,)), ((), ())),
        preferred_element_type=jnp.float32,
    )
    gate_conv_grad = hidden_grad * up_conv * gate_sigmoid * (1.0 + gate_conv * (1.0 - gate_sigmoid))
    up_conv_grad = hidden_grad * gate_act
    following = from_behind((gate_conv_grad[0:reach], up_conv_grad[0:reach]), "fs", -1)
    gate_grad_pad = jnp.concatenate([gate_conv_grad, following[0]], axis=0)
    up_grad_pad = jnp.concatenate([up_conv_grad, following[1]], axis=0)
    gate_grad = gate_taps_f[0] * gate_grad_pad[reach : reach + row_count]
    up_grad = up_taps_f[0] * up_grad_pad[reach : reach + row_count]
    for offset in range(1, tap_count):
        lead = reach - offset
        gate_grad = gate_grad + gate_taps_f[offset] * gate_grad_pad[lead : lead + row_count]
        up_grad = up_grad + up_taps_f[offset] * up_grad_pad[lead : lead + row_count]
    gate_tap_terms = jnp.stack(
        [
            jnp.sum(gate_conv_grad * gate_padded[offset : offset + row_count], axis=0)
            for offset in range(tap_count)
        ]
    )
    up_tap_terms = jnp.stack(
        [
            jnp.sum(up_conv_grad * up_padded[offset : offset + row_count], axis=0)
            for offset in range(tap_count)
        ]
    )
    tap_terms = jnp.stack([gate_tap_terms, up_tap_terms])
    feature_count = whole_cot.shape[1]
    down_grad = own_rows.T
    partial_norms = jnp.sum(own_rows * own_rows, axis=0)
    tap_rows = tap_terms.reshape(2 * tap_count, channels)
    pad = -(2 * tap_count + 1) % 8
    mine = jnp.concatenate(
        [tap_rows, partial_norms[None], jnp.zeros((pad, channels), jnp.float32)], axis=0
    )
    summed, everywhere = small_sums(mine)
    row_norms = summed[2 * tap_count] / feature_count
    tap_grads = (
        everywhere[:, : 2 * tap_count].transpose(1, 0, 2).reshape(2, tap_count, -1) * grad_scale
    )
    return (
        gate_grad.astype(jnp.bfloat16),
        up_grad.astype(jnp.bfloat16),
        down_grad,
        row_norms,
        tap_grads,
    )


PIECES = 4
ROW_TILE = 128
SUB = 32
BLOCK = 64
LANES = 128
BF16_ROWS = 16


def cut(channels):
    tiles = channels // LANES
    sizes = [(tiles + PIECES - 1 - i) // PIECES * LANES for i in range(PIECES)]
    return [(sum(sizes[:i]), sizes[i]) for i in range(PIECES)]


def less(a, b):
    return (b - a - 1 + 4096) // 4096


def whole_kernel(
    chips,
    tps,
    scale,
    gate_ref,
    up_ref,
    gtaps_ref,
    utaps_ref,
    down_ref,
    cot_ref,
    gate_out,
    up_out,
    down_out,
    norm_out,
    taps_out,
    gate_v,
    up_v,
    tap_in,
    taps_v,
    a_v,
    b_v,
    hid_t,
    cot_v,
    down_v,
    pair_send,
    pair_recv,
    rs_recv,
    rs_send,
    own_v,
    hg_v,
    edge_send,
    edge_recv,
    acc_v,
    tap_mine,
    tap_pair,
    tap_chip,
    tap_all,
    norm_all,
    norm_v,
    *sems,
):
    (local, z_send, z_recv, pd_send, pd_recv, pt_send, pt_recv, c_send, c_recv) = sems[:9]
    (h_send, h_recv, e_send, e_recv, tp_send, tp_recv, tz_send, tz_recv) = sems[9:17]
    (ta_send, ta_recv, n_send, n_recv, down_sem) = sems[17:]
    f, q = lax.axis_index("fs"), lax.axis_index("tp")
    z, core = f // 2, f % 2
    fs = 2 * chips
    partner = z * 2 + 1 - core
    rows, features = cot_ref.shape
    channels, cols = down_ref.shape
    total_rows = rows * tps
    chip_cols = 2 * cols
    pieces = cut(channels)
    lane_tiles = channels // LANES
    half = z // (chips // 2)
    width = math.isqrt(tps)
    spot = snake(q, width)
    half_ring = tps // 2
    ring_next = (snake((spot + 1) % tps, width), snake((spot + tps - 1) % tps, width))
    f32, bf16 = jnp.float32, jnp.bfloat16

    def remote(src, dst, send, recv, device):
        return pltpu.make_async_remote_copy(
            src_ref=src,
            dst_ref=dst,
            send_sem=send,
            recv_sem=recv,
            device_id=device,
            device_id_type=MESH,
        )

    def down_piece(chip, which, s):
        col = pl.multiple_of(chip * chip_cols + which * cols, cols)
        return down_v.at[pl.ds(*pieces[s]), pl.ds(col, cols)]

    own_cot = pltpu.make_async_copy(
        cot_ref, cot_v.at[pl.ds(pl.multiple_of(q * rows, rows), rows)], local.at[0]
    )
    own_down = pltpu.make_async_copy(
        down_ref,
        down_v.at[:, pl.ds(pl.multiple_of(f * cols, cols), cols)],
        local.at[1],
    )
    load_gate = pltpu.make_async_copy(
        gate_ref, gate_v.at[pl.ds(BF16_ROWS, total_rows)], local.at[2]
    )
    load_up = pltpu.make_async_copy(up_ref, up_v.at[pl.ds(BF16_ROWS, total_rows)], local.at[3])
    tap_col = pl.ds(pl.multiple_of(q * channels, LANES), channels)
    load_taps = [
        pltpu.make_async_copy(ref.at[:, tap_col], tap_in.at[b], local.at[7 + b])
        for b, ref in enumerate((gtaps_ref, utaps_ref))
    ]
    own_down.start()
    own_cot.start()
    load_taps[0].start()
    load_taps[1].start()
    load_gate.start()
    load_up.start()

    barrier = pltpu.get_barrier_semaphore()
    for i in range(1, fs):
        pl.semaphore_signal(barrier, inc=1, device_id={"fs": (f + i) % fs}, device_id_type=MESH)
    for i in range(1, tps):
        pl.semaphore_signal(barrier, inc=1, device_id={"tp": (q + i) % tps}, device_id_type=MESH)
    for i in range(1, tps):
        pl.semaphore_signal(
            barrier,
            inc=1,
            device_id={"fs": partner, "tp": (q + i) % tps},
            device_id_type=MESH,
        )
    pl.semaphore_wait(barrier, fs + 2 * tps - 3)

    def chip_at(position, way):
        return position + way * (chips - 1 - 2 * position)

    def z_copy(src, dst, way, p, s):
        return remote(
            src,
            dst,
            z_send.at[way, p, s],
            z_recv.at[way, p, s],
            {"fs": (f + 2 * (1 - 2 * way) + fs) % fs},
        )

    def pair_down(chip, which, s):
        where = down_piece(chip, which, s)
        return remote(where, where, pd_send.at[chip, s], pd_recv.at[chip, s], {"fs": partner})

    def halo_copy(i, src, dst):
        return remote(
            src.at[pl.ds(total_rows - BF16_ROWS, BF16_ROWS)],
            dst.at[pl.ds(0, BF16_ROWS)],
            h_send.at[i],
            h_recv.at[i],
            {"fs": (f + 1) % fs},
        )

    def chunk_chip(k):
        near = z + half * (chips - 1 - 2 * z)
        if k == chips - 1:
            position = near
        else:
            far = chips - 1 - near
            first = less(k, far)
            position = first * (chips - 1 - k) + (1 - first) * (k - far)
        return position + half * (chips - 1 - 2 * position)

    def cot_part(owner_spot, way, part, k):
        owner = snake((owner_spot + 2 * tps) % tps, width)
        col = pl.ds(pl.multiple_of(chunk_chip(k) * chip_cols, chip_cols), chip_cols)
        if part:
            start = owner * rows + way * (rows // 2)
            return cot_v.at[pl.ds(pl.multiple_of(start, rows // 2), rows // 2), col]
        return cot_v.at[pl.ds(pl.multiple_of(owner * rows, rows), rows), col]

    def ring_copy(k, step, way):
        sign = 1 - 2 * way
        where = cot_part(spot - sign * (step - 1), way, step == half_ring, k)
        return remote(
            where,
            where,
            c_send.at[k, way, step - 1],
            c_recv.at[k, way, step - 1],
            {"tp": ring_next[way]},
        )

    def ring_landing(k, step, way):
        sign = 1 - 2 * way
        where = cot_part(spot - sign * step, way, step == half_ring, k)
        return remote(
            where,
            where,
            c_send.at[k, way, step - 1],
            c_recv.at[k, way, step - 1],
            {"tp": ring_next[way]},
        )

    def ring_step(k, step):
        for way in range(2):
            ring_landing(k, step, way).wait_recv()
            if step < half_ring:
                ring_copy(k, step + 1, way).start()
        if step == 1:
            for ahead in range(1 + min(k, 1), 3):
                if k + ahead < chips:
                    for way in range(2):
                        ring_copy(k + ahead, 1, way).start()

    own_down.wait()

    @pl.when(f < fs - 1)
    def _():
        halo_copy(0, gate_ref, gate_v).start()
        halo_copy(1, up_ref, up_v).start()

    for s in range(PIECES):
        where = down_piece(z, core, s)

        @pl.when(z < chips - 1)
        def _():
            z_copy(where, where, 0, 0, s).start()

        @pl.when(z > 0)
        def _():
            z_copy(where, where, 1, 0, s).start()

    own_cot.wait()
    for way in range(2):
        ring_copy(0, 1, way).start()
    for s in range(PIECES):
        pair_down(z, core, s).start()

    for b in range(2):
        load_taps[b].wait()
        taps_v[b, 0:3, :] = tap_in[b].astype(f32)

    def hidden_tile(tile, lane_tile):
        lane = pl.ds(pl.multiple_of(lane_tile * LANES, LANES), LANES)
        gt = [taps_v[0, k : k + 1, lane] for k in range(3)]
        ut = [taps_v[1, k : k + 1, lane] for k in range(3)]
        parts = []
        for i in range(ROW_TILE // SUB):
            start = pl.multiple_of(tile * ROW_TILE + i * SUB, SUB)
            window = pl.ds(start, SUB + BF16_ROWS)
            g = gate_v[window, lane].astype(f32)
            u = up_v[window, lane].astype(f32)
            g_conv = (
                gt[0] * pltpu.roll(g, 2, 0)[BF16_ROWS:]
                + gt[1] * pltpu.roll(g, 1, 0)[BF16_ROWS:]
                + gt[2] * g[BF16_ROWS:]
            )
            u_conv = (
                ut[0] * pltpu.roll(u, 2, 0)[BF16_ROWS:]
                + ut[1] * pltpu.roll(u, 1, 0)[BF16_ROWS:]
                + ut[2] * u[BF16_ROWS:]
            )
            sig = 0.5 * jnp.tanh(0.5 * g_conv) + 0.5
            act = g_conv * sig
            out = pl.ds(start, SUB)
            a_v[out, lane] = u_conv * (sig + act * (1.0 - sig))
            b_v[out, lane] = act
            parts.append((act * u_conv).astype(bf16))
        tile_t = jnp.concatenate(parts, axis=0).T
        hid_t[lane, pl.ds(pl.multiple_of(tile * ROW_TILE, ROW_TILE), ROW_TILE)] = tile_t

    tiles = total_rows // ROW_TILE

    def hidden_piece(s, first, count):
        start, size = pieces[s]
        lane_count = size // LANES

        def step(i, carry):
            hidden_tile(first + i // lane_count, start // LANES + i % lane_count)
            return carry

        lax.fori_loop(0, count * lane_count, step, 0)

    load_gate.wait()
    load_up.wait()
    hidden_piece(0, 1, tiles - 1)
    hidden_piece(1, 1, tiles - 1)

    @pl.when(f > 0)
    def _():
        halo_copy(0, gate_ref, gate_v).wait_recv()
        halo_copy(1, up_ref, up_v).wait_recv()

    @pl.when(f == 0)
    def _():
        gate_v[0:BF16_ROWS, :] = jnp.zeros((BF16_ROWS, channels), bf16)
        up_v[0:BF16_ROWS, :] = jnp.zeros((BF16_ROWS, channels), bf16)

    hidden_piece(0, 0, 1)
    hidden_piece(1, 0, 1)
    ring_step(0, 1)
    hidden_piece(2, 0, tiles)
    hidden_piece(3, 0, tiles)

    def pair_terms_copy(chip, s):
        here = pl.ds(*pieces[s])
        return remote(
            pair_send.at[chip, here],
            pair_recv.at[chip, here],
            pt_send.at[chip, s],
            pt_recv.at[chip, s],
            {"fs": partner},
        )

    def pair_terms(k):
        chip = chunk_chip(k)
        both = cot_v[:, pl.ds(pl.multiple_of(chip * chip_cols, chip_cols), chip_cols)]
        mid = PIECES // 2
        for group in (range(mid), range(mid, PIECES)):
            start = pieces[group[0]][0]
            size = sum(pieces[s][1] for s in group)
            here = pl.ds(start, size)
            value = jnp.dot(hid_t[here, :], both, preferred_element_type=f32)
            low, high = value[:, :cols], value[:, cols:]
            pair_send[chip, here, :] = jnp.where(core == 0, high, low).astype(bf16)
            for s in group:
                pair_terms_copy(chip, s).start()
            own_v[chip, here, :] = jnp.where(core == 0, low, high)

    def pair_terms_wait(k, s):
        pair_terms_copy(chunk_chip(k), s).wait_recv()

    def send_sum(position, way, p, s, first):
        chip = chip_at(chips - 1 + position - p, way)
        here = pl.ds(*pieces[s])
        value = own_v[chip, here, :] + pair_recv[chip, here, :].astype(f32)
        if not first:
            value = value + rs_recv[way, chip, here, :].astype(f32)
        rs_send[chip, here, :] = value.astype(bf16)
        z_copy(rs_send.at[chip, here], rs_recv.at[way, chip, here], way, p + 1, s).start()

    def both_ways(body):
        def step(d, carry):
            way = (half + d) % 2
            body(way, z + way * (chips - 1 - 2 * z))
            return carry

        lax.fori_loop(0, 2, step, 0)

    def first_sum(p, s):
        def body(way, position):
            @pl.when(position == 0)
            def _():
                send_sum(position, way, p, s, True)

        both_ways(body)

    def slot(p, s, arrive=True, send=True):
        here = pl.ds(*pieces[s])

        def body(way, position):
            if arrive:

                @pl.when(position > p)
                def _():
                    chip = chip_at(position - 1 - p, way)
                    where = down_piece(chip, core, s)
                    z_copy(where, where, way, p, s).wait_recv()
                    if p + 1 < chips:

                        @pl.when(position < chips - 1)
                        def _():
                            z_copy(where, where, way, p + 1, s).start()

                    pair_down(chip, core, s).start()

            if p > 0:
                if arrive:

                    @pl.when(jnp.logical_and(position > 0, position <= p))
                    def _():
                        chip = chip_at(chips - 1 + position - p, way)
                        where = rs_recv.at[way, chip, here]
                        z_copy(where, where, way, p, s).wait_recv()

                if send and p + 1 < chips:

                    @pl.when(jnp.logical_and(position > 0, position <= p))
                    def _():
                        send_sum(position, way, p, s, False)

        both_ways(body)

    def pair_down_wait(chip):
        for s in range(PIECES):
            pair_down(chip, 1 - core, s).wait_recv()

    last_chip = (1 - half) * (chips - 1)

    def hidden_grad(first_chip, count, add):
        depth = count * chip_cols
        col = pl.ds(pl.multiple_of(first_chip * chip_cols, chip_cols), depth)

        def one(start, size):
            lane = pl.ds(start, size)
            value = lax.dot_general(
                cot_v[:, col],
                down_v[lane, col],
                (((1,), (1,)), ((), ())),
                preferred_element_type=f32,
            )
            if add:
                value = value + hg_v[0:total_rows, lane]
            hg_v[0:total_rows, lane] = value

        wide = 2 * LANES

        def step(n, carry):
            one(pl.multiple_of(n * wide, wide), wide)
            return carry

        lax.fori_loop(0, channels // wide, step, 0)
        if channels % wide:
            one(channels - channels % wide, channels % wide)

    def ring_ends(k):
        for step in range(2, half_ring + 1):
            ring_step(k, step)

    def ready(k):
        ring_ends(k)
        pair_terms(k)

    def start_sums(k):
        for s in range(PIECES):
            pair_terms_wait(k, s)
            first_sum(k, s)

    mid = PIECES // 2
    for s in range(mid):
        slot(0, s)
    ready(0)
    start_sums(0)
    for s in range(mid, PIECES):
        slot(0, s)
    ring_step(1, 1)
    for p in range(1, chips - 2):
        slot(p, 0)
        ring_step(p + 1, 1)
        ring_ends(p)
        for s in range(1, mid):
            slot(p, s)
        pair_terms(p)
        start_sums(p)
        for s in range(mid, PIECES):
            slot(p, s)
    ring_step(chips - 1, 1)
    ready(chips - 2)
    for s in range(mid):
        pair_terms_wait(chips - 2, s)
    slot(chips - 2, 0)
    first_sum(chips - 2, 0)
    ready(chips - 1)
    for i in range(chips - 1):
        pair_down_wait(half + i)
    hidden_grad(half, chips - 1, False)
    for s in range(1, mid):
        first_sum(chips - 2, s)
    for s in range(PIECES):
        pair_terms_wait(chips - 1, s)
    for s in range(1, mid):
        slot(chips - 2, s)
    for s in range(mid, PIECES):
        slot(chips - 2, s, send=False)
    pair_down_wait(last_chip)
    hidden_grad(last_chip, 1, True)

    edge = 8
    row_index = lax.broadcasted_iota(jnp.int32, (edge, channels), 0)
    top = pl.ds(0, edge)
    edge_send[...] = jnp.where(
        row_index < 2,
        hg_v[top, :] * a_v[top, :],
        pltpu.roll(hg_v[top, :] * b_v[top, :], 2, 0),
    )
    edge_copy = remote(
        edge_send, edge_recv, e_send.at[0], e_recv.at[0], {"fs": (f + fs - 1) % fs}
    )

    @pl.when(f > 0)
    def _():
        edge_copy.start()

    for s in range(mid, PIECES):
        pair_terms_wait(chips - 2, s)
        first_sum(chips - 2, s)
        slot(chips - 2, s, arrive=False)

    def grads(start, lane, sums):
        window = pl.ds(start, BLOCK + edge)
        here = pl.ds(pl.multiple_of(start + BF16_ROWS, BF16_ROWS), BLOCK)
        hg = hg_v[window, lane]
        new = []
        for b, (factor, pre) in enumerate(((a_v, gate_v), (b_v, up_v))):
            g = hg * factor[window, lane]
            g0 = g[0:BLOCK]
            g1 = pltpu.roll(g, BLOCK + edge - 1, 0)[0:BLOCK]
            g2 = pltpu.roll(g, BLOCK + edge - 2, 0)[0:BLOCK]
            x = pre[here, lane].astype(f32)
            for i, shifted in enumerate((g2, g1, g0)):
                product = (shifted * x).reshape(BLOCK // 8, 8, LANES)
                new.append(sums[3 * b + i] + jnp.sum(product, axis=0))
            t = [taps_v[b, k : k + 1, lane] for k in range(3)]
            pre[here, lane] = (t[0] * g2 + t[1] * g1 + t[2] * g0).astype(bf16)
        return tuple(new)

    blocks = total_rows // BLOCK

    def grad_lanes(lane_tile, carry):
        lane = pl.ds(pl.multiple_of(lane_tile * LANES, LANES), LANES)

        def step(i, sums):
            return grads(pl.multiple_of(i * BLOCK, BLOCK), lane, sums)

        zero = jnp.zeros((8, LANES), f32)
        sums = lax.fori_loop(0, blocks - 1, step, (zero,) * 6)
        for i in range(6):
            acc_v[i, :, lane] = sums[i]
        return carry

    def grad_last(lane_tile, carry):
        lane = pl.ds(pl.multiple_of(lane_tile * LANES, LANES), LANES)
        sums = grads((blocks - 1) * BLOCK, lane, tuple(acc_v[i, :, lane] for i in range(6)))
        for b in range(2):
            for k in range(3):
                tap_mine[b, k : k + 1, lane] = jnp.sum(sums[3 * b + k], axis=0, keepdims=True)
        return carry

    lax.fori_loop(0, lane_tiles // 2, grad_lanes, 0)
    lax.fori_loop(lane_tiles // 2, lane_tiles, grad_lanes, 0)

    @pl.when(f < fs - 1)
    def _():
        edge_copy.wait_recv()

    @pl.when(f == fs - 1)
    def _():
        edge_recv[...] = jnp.zeros((edge, channels), f32)

    bottom = pl.ds(total_rows, edge)
    hg_v[bottom, :] = jnp.ones((edge, channels), f32)
    a_v[bottom, :] = edge_recv[...]
    b_v[bottom, :] = pltpu.roll(edge_recv[...], edge - 2, 0)
    tap_mine[...] = jnp.zeros(tap_mine.shape, f32)
    lax.fori_loop(0, lane_tiles, grad_last, 0)
    store_gate = pltpu.make_async_copy(
        gate_v.at[pl.ds(BF16_ROWS, total_rows)], gate_out, local.at[4]
    )
    store_up = pltpu.make_async_copy(up_v.at[pl.ds(BF16_ROWS, total_rows)], up_out, local.at[5])
    store_gate.start()
    store_up.start()

    def store_down(s):
        here = pl.ds(*pieces[s])
        return pltpu.make_async_copy(own_v.at[z, here], down_out.at[here], down_sem.at[s])

    tap_pair_copy = remote(
        tap_mine.at[1 - core], tap_pair, tp_send.at[0], tp_recv.at[0], {"fs": partner}
    )
    tap_pair_copy.start()

    def tap_chip_copy(i, sender):
        return remote(
            tap_chip.at[sender],
            tap_chip.at[sender],
            tz_send.at[i],
            tz_recv.at[sender],
            {"fs": ((z + i) % chips) * 2 + core},
        )

    tap_pair_copy.wait_recv()
    tap_chip[z] = tap_mine[core] + tap_pair[...]
    for i in range(1, chips):
        tap_chip_copy(i, z).start()

    ones = jnp.ones((8, cols), bf16)
    contract = (((1,), (1,)), ((), ()))
    for s in range(PIECES):
        slot(chips - 1, s)
        here = pl.ds(*pieces[s])
        value = own_v[z, here, :] + pair_recv[z, here, :].astype(f32)
        value = value + jnp.where(z > 0, rs_recv[0, z, here, :].astype(f32), 0.0)
        value = value + jnp.where(z < chips - 1, rs_recv[1, z, here, :].astype(f32), 0.0)
        value = value * scale
        own_v[z, here, :] = value
        store_down(s).start()
        square = value * value
        high = square.astype(bf16)
        low = (square - high.astype(f32)).astype(bf16)
        norm = lax.dot_general(ones, high, contract, preferred_element_type=f32)
        norm = norm + lax.dot_general(ones, low, contract, preferred_element_type=f32)
        norm_all[f, :, here] = norm[0:1]

    def norm_copy(i, sender):
        return remote(
            norm_all.at[sender],
            norm_all.at[sender],
            n_send.at[i],
            n_recv.at[sender],
            {"fs": (f + i) % fs},
        )

    for i in range(1, fs):
        norm_copy(i, f).start()
    @pl.when(f < fs - 1)
    def _():
        halo_copy(0, gate_ref, gate_v).wait_send()
        halo_copy(1, up_ref, up_v).wait_send()

    @pl.when(f > 0)
    def _():
        edge_copy.wait_send()

    for k in range(chips):
        for way in range(2):
            for step in range(1, half_ring + 1):
                ring_copy(k, step, way).wait_send()
        for s in range(PIECES):
            pair_terms_copy(k, s).wait_send()
        for s in range(PIECES):
            pair_down(k, core, s).wait_send()

    for p in range(chips):
        for s in range(PIECES):
            where = rs_send.at[0, pl.ds(*pieces[s])]

            @pl.when(z < chips - 1)
            def _():
                z_copy(where, where, 0, p, s).wait_send()

            @pl.when(z > 0)
            def _():
                z_copy(where, where, 1, p, s).wait_send()

    for i in range(1, chips):
        tap_chip_copy(i, (z + i) % chips).wait_recv()
    total = tap_chip[0]
    for i in range(1, chips):
        total = total + tap_chip[i]
    tap_all[core, q] = total * scale

    def tap_all_copy(j, i, which, sender):
        to = core if j == 0 else 1 - core
        return remote(
            tap_all.at[which, sender],
            tap_all.at[which, sender],
            ta_send.at[j, i],
            ta_recv.at[which, sender],
            {"fs": z * 2 + to, "tp": (q + i) % tps},
        )

    others = [(j, i) for i in range(tps) for j in range(2) if (j, i) != (0, 0)]
    for j, i in others:
        tap_all_copy(j, i, core, q).start()
    for i in range(1, fs):
        norm_copy(i, (f + i) % fs).wait_recv()
    total = norm_all[0]
    for i in range(1, fs):
        total = total + norm_all[i]
    norm_v[...] = total * (1.0 / features)
    store_norm = pltpu.make_async_copy(norm_v, norm_out, local.at[9])
    store_norm.start()
    for j, i in others:
        which = core if j == 0 else 1 - core
        tap_all_copy(j, i, which, (q + i) % tps).wait_recv()
    store_taps = pltpu.make_async_copy(tap_all, taps_out, local.at[10])
    store_taps.start()

    store_norm.wait()
    store_taps.wait()
    store_gate.wait()
    store_up.wait()
    for s in range(PIECES):
        store_down(s).wait()

    tap_pair_copy.wait_send()
    for i in range(1, chips):
        tap_chip_copy(i, z).wait_send()
    for j, i in others:
        tap_all_copy(j, i, core, q).wait_send()
    for i in range(1, fs):
        norm_copy(i, f).wait_send()


def hand_over_kernel(*refs):
    gate_ref, up_ref, down_ref, norm_ref, taps_ref = refs[:5]
    gate_out, up_out, down_out, norm_out, taps_out = refs[5:10]
    gate_v, up_v, down_v, sem_in, sem_out = refs[10:]
    moves = []
    for src, mid, dst in (
        (gate_ref, gate_v, gate_out),
        (up_ref, up_v, up_out),
        (down_ref, down_v, down_out),
    ):
        rows = src.shape[0]
        parts = 4 if src.shape[0] % 64 == 0 else 1
        for i in range(parts):
            here = pl.ds(i * (rows // parts), rows // parts)
            moves.append((src.at[here], mid.at[here], dst.at[here]))
    first = [
        pltpu.make_async_copy(src, mid, sem_in.at[i]) for i, (src, mid, _) in enumerate(moves)
    ]
    second = [
        pltpu.make_async_copy(mid, dst, sem_out.at[i]) for i, (_, mid, dst) in enumerate(moves)
    ]
    for copy in first:
        copy.start()
    channels = norm_ref.shape[1]
    norm_out[...] = norm_ref[...]
    for b in range(2):
        for k in range(3):
            for i in range(taps_ref.shape[1]):
                taps_out[k, b : b + 1, i * channels : (i + 1) * channels] = taps_ref[
                    b, i, k : k + 1, :
                ]
    for copy, after in zip(first, second):
        copy.wait()
        after.start()
    for copy in second:
        copy.wait()


def hand_over(gate_grad, up_grad, down_grad, norms, taps):
    tps, channels = taps.shape[1], taps.shape[3]
    dma = pltpu.SemaphoreType.DMA
    big = (gate_grad, up_grad, down_grad)
    return pl.pallas_call(
        hand_over_kernel,
        out_shape=tuple(jax.ShapeDtypeStruct(a.shape, a.dtype) for a in big)
        + (
            jax.ShapeDtypeStruct((1, channels), jnp.float32),
            jax.ShapeDtypeStruct((3, 2, channels * tps), jnp.float32),
        ),
        in_specs=[pl.BlockSpec(memory_space=pl.ANY)] * 3
        + [pl.BlockSpec(memory_space=pltpu.VMEM)] * 2,
        out_specs=[pl.BlockSpec(memory_space=pl.ANY)] * 3
        + [pl.BlockSpec(memory_space=pltpu.VMEM)] * 2,
        scratch_shapes=[pltpu.VMEM(a.shape, a.dtype) for a in big] + [dma((12,)), dma((12,))],
        name="hand_over",
    )(*big, norms, taps)


def whole_body(gate_pre, up_pre, gate_taps, up_taps, down_proj, cotangent):
    fs, tps = lax.axis_size("fs"), lax.axis_size("tp")
    chips = fs // 2
    rows, features = cotangent.shape
    channels, cols = down_proj.shape
    total = rows * tps
    f32, bf16 = jnp.float32, jnp.bfloat16
    dma = pltpu.SemaphoreType.DMA
    scale = 1.0 / math.sqrt(total * fs)
    ring = (chips, 2, tps // 2)
    gate_grad, up_grad, down_grad, norms, taps = pl.pallas_call(
        functools.partial(whole_kernel, chips, tps, scale),
        out_shape=(
            jax.ShapeDtypeStruct((total, channels), bf16),
            jax.ShapeDtypeStruct((total, channels), bf16),
            jax.ShapeDtypeStruct((channels, cols), f32),
            jax.ShapeDtypeStruct((1, channels), f32),
            jax.ShapeDtypeStruct((2, tps, 4, channels), f32),
        ),
        in_specs=[
            pl.BlockSpec(memory_space=pl.ANY)
        ]
        * 6,
        out_specs=[pl.BlockSpec(memory_space=pl.ANY)] * 5,
        scratch_shapes=[
            pltpu.VMEM((total + BF16_ROWS, channels), bf16),
            pltpu.VMEM((total + BF16_ROWS, channels), bf16),
            pltpu.VMEM((2, 3, channels), bf16),
            pltpu.VMEM((2, 4, channels), f32),
            pltpu.VMEM((total + 8, channels), f32),
            pltpu.VMEM((total + 8, channels), f32),
            pltpu.VMEM((channels, total), bf16),
            pltpu.VMEM((total, features), bf16),
            pltpu.VMEM((channels, features), bf16),
            pltpu.VMEM((chips, channels, cols), bf16),
            pltpu.VMEM((chips, channels, cols), bf16),
            pltpu.VMEM((2, chips, channels, cols), bf16),
            pltpu.VMEM((chips, channels, cols), bf16),
            pltpu.VMEM((chips, channels, cols), f32),
            pltpu.VMEM((total + 8, channels), f32),
            pltpu.VMEM((8, channels), f32),
            pltpu.VMEM((8, channels), f32),
            pltpu.VMEM((6, 8, channels), f32),
            pltpu.VMEM((2, 4, channels), f32),
            pltpu.VMEM((4, channels), f32),
            pltpu.VMEM((chips, 4, channels), f32),
            pltpu.VMEM((2, tps, 4, channels), f32),
            pltpu.VMEM((fs, 1, channels), f32),
            pltpu.VMEM((1, channels), f32),
            dma((11,)),
            dma((2, chips, PIECES)),
            dma((2, chips, PIECES)),
            dma((chips, PIECES)),
            dma((chips, PIECES)),
            dma((chips, PIECES)),
            dma((chips, PIECES)),
            dma(ring),
            dma(ring),
            dma((2,)),
            dma((2,)),
            dma((1,)),
            dma((1,)),
            dma((1,)),
            dma((1,)),
            dma((chips,)),
            dma((chips,)),
            dma((2, tps)),
            dma((2, tps)),
            dma((fs,)),
            dma((fs,)),
            dma((PIECES,)),
        ],
        compiler_params=pltpu.CompilerParams(
            collective_id=2, has_side_effects=True, vmem_limit_bytes=VMEM_BYTES
        ),
        name="whole_layer",
    )(gate_pre, up_pre, gate_taps, up_taps, down_proj, cotangent)
    gate_grad, up_grad, down_grad, norms, taps = hand_over(
        gate_grad, up_grad, down_grad, norms, taps
    )
    return gate_grad, up_grad, down_grad, norms.reshape(channels), taps.transpose(1, 0, 2)


VMEM_BYTES = 64_000_000
SPARE_BYTES = 5_000_000


def fits_whole(gate_pre, gate_taps, down_proj, cotangent):
    fs, tps = lax.axis_size("fs"), lax.axis_size("tp")
    chips = fs // 2
    channels, cols = down_proj.shape
    rows, features = cotangent.shape
    total = rows * tps
    tiled = channels % LANES == 0 and cols % (2 * LANES) == 0
    tiled = tiled and channels >= LANES * PIECES and total % ROW_TILE == 0
    tiled = tiled and rows % (2 * BF16_ROWS) == 0 and gate_taps.shape[0] == 3
    tiled = tiled and fs % 2 == 0 and chips % 2 == 0 and chips >= 4 and tps >= 4
    held = 2 * total * channels * (2 + 4) + total * channels * (2 + 4)
    held += (total + channels) * features * 2 + channels * cols * chips * (5 * 2 + 4)
    return tiled and held + SPARE_BYTES < VMEM_BYTES


def body(gate_pre, up_pre, gate_taps, up_taps, down_proj, cotangent):
    args = (gate_pre, up_pre, gate_taps, up_taps, down_proj, cotangent)
    if fits_whole(gate_pre, gate_taps, down_proj, cotangent):
        return whole_body(*args)
    return staged_body(*args)


def solution(mesh):
    placed = (P("fs", "tp"), P("fs", "tp"), P(), P(), P("tp", "fs"), P(("fs", "tp"), None))
    return jax.shard_map(
        body,
        mesh=mesh,
        in_specs=placed,
        out_specs=(P("fs", "tp"), P("fs", "tp"), P("tp", "fs"), P("tp"), P()),
        check_vma=False,
    )
```

```python
import functools
import math

import jax
import jax.numpy as jnp
from jax import lax
from jax.experimental import pallas as pl
from jax.experimental.pallas import tpu as pltpu
from jax.sharding import PartitionSpec as P

MESH = pl.DeviceIdType.MESH


def snake(position, width):
    row, column = position // width, position % width
    return row * width + column + (row % 2) * (width - 1 - 2 * column)


def gather_kernel(chips, tps, cot_ref, down_ref, cot_out, down_out, *sems):
    (ring_send, ring_recv, line_send, line_recv, pair_send, pair_recv, local_sem) = sems
    f, q = lax.axis_index("fs"), lax.axis_index("tp")
    z, core = f // 2, f % 2
    width = math.isqrt(tps)
    spot = snake(q, width)
    half_ring = tps // 2
    ring_next = (snake((spot + 1) % tps, width), snake((spot + tps - 1) % tps, width))
    rows = cot_ref.shape[0]
    cols = down_ref.shape[1]
    partner = z * 2 + 1 - core
    behind, ahead = z > 0, z < chips - 1

    barrier = pltpu.get_barrier_semaphore()
    for device in ({"tp": ring_next[0]}, {"tp": ring_next[1]}, {"fs": partner}):
        pl.semaphore_signal(barrier, inc=1, device_id=device, device_id_type=MESH)

    @pl.when(behind)
    def _():
        pl.semaphore_signal(barrier, inc=1, device_id={"fs": f - 2}, device_id_type=MESH)

    @pl.when(ahead)
    def _():
        pl.semaphore_signal(barrier, inc=1, device_id={"fs": f + 2}, device_id_type=MESH)

    pl.semaphore_wait(barrier, 4 + (z + chips - 1) // chips - (z + 1) // chips)

    def cot_rows(owner_spot, way, part):
        owner = snake((owner_spot + 2 * tps) % tps, width)
        if part:
            return pl.ds(owner * rows + way * (rows // 2), rows // 2)
        return pl.ds(owner * rows, rows)

    def ring_copy(step, way):
        sign = 1 - 2 * way
        part = step == half_ring
        where = cot_rows(spot - sign * (step - 1), way, part)
        if step == 1:
            src = cot_ref.at[pl.ds(way * (rows // 2), rows // 2)] if part else cot_ref
        else:
            src = cot_out.at[where]
        return pltpu.make_async_remote_copy(
            src_ref=src,
            dst_ref=cot_out.at[where],
            send_sem=ring_send.at[way, step - 1],
            recv_sem=ring_recv.at[way, step - 1],
            device_id={"tp": ring_next[way]},
            device_id_type=MESH,
        )

    def ring_landing(step, way):
        sign = 1 - 2 * way
        where = cot_rows(spot - sign * step, way, step == half_ring)
        return pltpu.make_async_remote_copy(
            src_ref=cot_out.at[where],
            dst_ref=cot_out.at[where],
            send_sem=ring_send.at[way, step - 1],
            recv_sem=ring_recv.at[way, step - 1],
            device_id={"tp": ring_next[way]},
            device_id_type=MESH,
        )

    def down_block(chip, which):
        block = chip * 2 + which
        if cols % 128:
            return down_out.at[block]
        return down_out.at[:, pl.ds(pl.multiple_of(block * cols, cols), cols)]

    def line_copy(step, way):
        sign = 1 - 2 * way
        where = down_block(z - sign * (step - 1), core)
        return pltpu.make_async_remote_copy(
            src_ref=down_ref if step == 1 else where,
            dst_ref=where,
            send_sem=line_send.at[way, step - 1],
            recv_sem=line_recv.at[way, step - 1],
            device_id={"fs": f + 2 * sign},
            device_id_type=MESH,
        )

    def line_landing(step, way):
        sign = 1 - 2 * way
        where = down_block(z - sign * step, core)
        return pltpu.make_async_remote_copy(
            src_ref=where,
            dst_ref=where,
            send_sem=line_send.at[way, step - 1],
            recv_sem=line_recv.at[way, step - 1],
            device_id={"fs": f + 2 * sign},
            device_id_type=MESH,
        )

    def pair_copy(step, way, which):
        sign = 1 - 2 * way
        where = down_block(z - sign * step, which)
        slot = step + way * (chips - 1)
        return pltpu.make_async_remote_copy(
            src_ref=down_ref if step == 0 else where,
            dst_ref=where,
            send_sem=pair_send.at[slot],
            recv_sem=pair_recv.at[slot],
            device_id={"fs": partner},
            device_id_type=MESH,
        )

    def has_landing(step, way):
        return z >= step if way == 0 else z + step < chips

    def has_copy(step, way):
        going = ahead if way == 0 else behind
        return going if step == 1 else jnp.logical_and(going, has_landing(step - 1, way))

    for way in range(2):
        ring_copy(1, way).start()

        @pl.when(has_copy(1, way))
        def _():
            line_copy(1, way).start()

    pair_copy(0, 0, core).start()
    own_cot = pltpu.make_async_copy(cot_ref, cot_out.at[pl.ds(q * rows, rows)], local_sem.at[0])
    own_down = pltpu.make_async_copy(down_ref, down_block(z, core), local_sem.at[1])
    own_cot.start()
    own_down.start()

    for step in range(1, max(chips - 1, half_ring) + 1):
        if step <= chips - 1:
            for way in range(2):

                @pl.when(has_landing(step, way))
                def _():
                    line_landing(step, way).wait_recv()
                    pair_copy(step, way, core).start()

                if step + 1 <= chips - 1:

                    @pl.when(has_copy(step + 1, way))
                    def _():
                        line_copy(step + 1, way).start()

        if step <= half_ring:
            for way in range(2):
                ring_landing(step, way).wait_recv()
                if step + 1 <= half_ring:
                    ring_copy(step + 1, way).start()

    own_cot.wait()
    own_down.wait()
    pair_copy(0, 0, 1 - core).wait_recv()
    pair_copy(0, 0, core).wait_send()
    for way in range(2):
        for step in range(1, half_ring + 1):
            ring_copy(step, way).wait_send()
        for step in range(1, chips):

            @pl.when(has_copy(step, way))
            def _():
                line_copy(step, way).wait_send()

            @pl.when(has_landing(step, way))
            def _():
                pair_copy(step, way, 1 - core).wait_recv()
                pair_copy(step, way, core).wait_send()


def gather_both(cotangent, down_proj):
    fs, tps = lax.axis_size("fs"), lax.axis_size("tp")
    chips = fs // 2
    rows, features = cotangent.shape
    channels, cols = down_proj.shape
    dma = pltpu.SemaphoreType.DMA
    down_shape = (fs, channels, cols) if cols % 128 else (channels, cols * fs)
    whole_cot, whole_down = pl.pallas_call(
        functools.partial(gather_kernel, chips, tps),
        out_shape=(
            jax.ShapeDtypeStruct((rows * tps, features), cotangent.dtype),
            jax.ShapeDtypeStruct(down_shape, down_proj.dtype),
        ),
        in_specs=[pl.BlockSpec(memory_space=pltpu.VMEM)] * 2,
        out_specs=[pl.BlockSpec(memory_space=pl.ANY)] * 2,
        scratch_shapes=[
            dma((2, tps // 2)),
            dma((2, tps // 2)),
            dma((2, chips - 1)),
            dma((2, chips - 1)),
            dma((2 * chips - 1,)),
            dma((2 * chips - 1,)),
            dma((2,)),
        ],
        compiler_params=pltpu.CompilerParams(collective_id=0, has_side_effects=True),
        name="gather_both",
    )(cotangent, down_proj)
    if cols % 128:
        whole_down = whole_down.transpose(1, 0, 2).reshape(channels, fs * cols)
    return whole_cot, whole_down


def small_kernel(fs, tps, mine_ref, sum_ref, all_ref, terms, total, sums, *sems):
    send_a, recv_a, send_b, recv_b = sems
    f, q = lax.axis_index("fs"), lax.axis_index("tp")
    barrier = pltpu.get_barrier_semaphore()
    for i in range(1, fs):
        pl.semaphore_signal(
            barrier, inc=1, device_id={"fs": (f + i) % fs}, device_id_type=MESH
        )
    for i in range(1, tps):
        pl.semaphore_signal(
            barrier, inc=1, device_id={"tp": (q + i) % tps}, device_id_type=MESH
        )
    pl.semaphore_wait(barrier, fs + tps - 2)

    def over_fs(i):
        return pltpu.make_async_remote_copy(
            src_ref=mine_ref,
            dst_ref=terms.at[f],
            send_sem=send_a.at[i],
            recv_sem=recv_a.at[i],
            device_id={"fs": (f + i) % fs},
            device_id_type=MESH,
        )

    def over_tp(i):
        return pltpu.make_async_remote_copy(
            src_ref=total,
            dst_ref=sums.at[q],
            send_sem=send_b.at[i],
            recv_sem=recv_b.at[i],
            device_id={"tp": (q + i) % tps},
            device_id_type=MESH,
        )

    def landing(buffer, slot, send, recv, i, device):
        return pltpu.make_async_remote_copy(
            src_ref=buffer.at[slot],
            dst_ref=buffer.at[slot],
            send_sem=send.at[i],
            recv_sem=recv.at[i],
            device_id=device,
            device_id_type=MESH,
        )

    for i in range(1, fs):
        over_fs(i).start()
    terms[f] = mine_ref[...]
    for i in range(1, fs):
        landing(terms, (f + fs - i) % fs, send_a, recv_a, i, {"fs": (f + i) % fs}).wait_recv()
    added = terms[0]
    for i in range(1, fs):
        added = added + terms[i]
    total[...] = added
    sum_ref[...] = added
    sums[q] = added
    for i in range(1, fs):
        over_fs(i).wait_send()
    for i in range(1, tps):
        over_tp(i).start()
    for i in range(1, tps):
        landing(sums, (q + tps - i) % tps, send_b, recv_b, i, {"tp": (q + i) % tps}).wait_recv()
    all_ref[...] = sums[...]
    for i in range(1, tps):
        over_tp(i).wait_send()


def small_sums(mine):
    fs, tps = lax.axis_size("fs"), lax.axis_size("tp")
    dma = pltpu.SemaphoreType.DMA
    shape = mine.shape
    return pl.pallas_call(
        functools.partial(small_kernel, fs, tps),
        out_shape=(
            jax.ShapeDtypeStruct(shape, jnp.float32),
            jax.ShapeDtypeStruct((tps,) + shape, jnp.float32),
        ),
        in_specs=[pl.BlockSpec(memory_space=pltpu.VMEM)],
        out_specs=[pl.BlockSpec(memory_space=pltpu.VMEM)] * 2,
        scratch_shapes=[
            pltpu.VMEM((fs,) + shape, jnp.float32),
            pltpu.VMEM(shape, jnp.float32),
            pltpu.VMEM((tps,) + shape, jnp.float32),
            dma((fs,)),
            dma((fs,)),
            dma((tps,)),
            dma((tps,)),
        ],
        compiler_params=pltpu.CompilerParams(collective_id=1, has_side_effects=True),
        name="small_sums",
    )(mine)


def from_behind(block, axis, distance):
    devices = range(lax.axis_size(axis))
    route = [(i - distance, i) for i in devices if i - distance in devices]
    return lax.ppermute(block, axis, route)


def staged_body(gate_pre, up_pre, gate_taps, up_taps, down_proj, cotangent):
    row_count = gate_pre.shape[0]
    channels = gate_pre.shape[1]
    tap_count = gate_taps.shape[0]
    reach = tap_count - 1
    channel_start = lax.axis_index("tp") * channels
    gate_taps_f = lax.dynamic_slice_in_dim(gate_taps, channel_start, channels, 1).astype(
        jnp.float32
    )
    up_taps_f = lax.dynamic_slice_in_dim(up_taps, channel_start, channels, 1).astype(jnp.float32)
    before = from_behind((gate_pre[row_count - reach :], up_pre[row_count - reach :]), "fs", 1)
    gate_padded = jnp.concatenate([before[0], gate_pre], axis=0).astype(jnp.float32)
    up_padded = jnp.concatenate([before[1], up_pre], axis=0).astype(jnp.float32)
    gate_conv = gate_taps_f[0] * gate_padded[0:row_count]
    up_conv = up_taps_f[0] * up_padded[0:row_count]
    for offset in range(1, tap_count):
        gate_conv = gate_conv + gate_taps_f[offset] * gate_padded[offset : offset + row_count]
        up_conv = up_conv + up_taps_f[offset] * up_padded[offset : offset + row_count]
    gate_sigmoid = jax.nn.sigmoid(gate_conv)
    gate_act = gate_conv * gate_sigmoid
    hidden = (gate_act * up_conv).astype(jnp.bfloat16)
    hidden = lax.optimization_barrier(hidden)
    whole_cot, whole_down = gather_both(cotangent, down_proj)
    grad_scale = 1.0 / math.sqrt(row_count * lax.axis_size("fs"))
    sum_type = jnp.bfloat16 if lax.axis_size("fs") <= 8 else jnp.float32
    terms = lax.dot_general(
        whole_cot, hidden, (((0,), (0,)), ((), ())), preferred_element_type=jnp.float32
    ).astype(sum_type)
    terms, whole_down = lax.optimization_barrier((terms, whole_down))
    own_rows = lax.psum_scatter(terms, "fs", scatter_dimension=0, tiled=True)
    own_rows = own_rows.astype(jnp.float32) * grad_scale
    hidden_grad = lax.dot_general(
        whole_cot,
        whole_down,
        (((1,), (1,)), ((), ())),
        preferred_element_type=jnp.float32,
    )
    gate_conv_grad = hidden_grad * up_conv * gate_sigmoid * (1.0 + gate_conv * (1.0 - gate_sigmoid))
    up_conv_grad = hidden_grad * gate_act
    following = from_behind((gate_conv_grad[0:reach], up_conv_grad[0:reach]), "fs", -1)
    gate_grad_pad = jnp.concatenate([gate_conv_grad, following[0]], axis=0)
    up_grad_pad = jnp.concatenate([up_conv_grad, following[1]], axis=0)
    gate_grad = gate_taps_f[0] * gate_grad_pad[reach : reach + row_count]
    up_grad = up_taps_f[0] * up_grad_pad[reach : reach + row_count]
    for offset in range(1, tap_count):
        lead = reach - offset
        gate_grad = gate_grad + gate_taps_f[offset] * gate_grad_pad[lead : lead + row_count]
        up_grad = up_grad + up_taps_f[offset] * up_grad_pad[lead : lead + row_count]
    gate_tap_terms = jnp.stack(
        [
            jnp.sum(gate_conv_grad * gate_padded[offset : offset + row_count], axis=0)
            for offset in range(tap_count)
        ]
    )
    up_tap_terms = jnp.stack(
        [
            jnp.sum(up_conv_grad * up_padded[offset : offset + row_count], axis=0)
            for offset in range(tap_count)
        ]
    )
    tap_terms = jnp.stack([gate_tap_terms, up_tap_terms])
    feature_count = whole_cot.shape[1]
    down_grad = own_rows.T
    partial_norms = jnp.sum(own_rows * own_rows, axis=0)
    tap_rows = tap_terms.reshape(2 * tap_count, channels)
    pad = -(2 * tap_count + 1) % 8
    mine = jnp.concatenate(
        [tap_rows, partial_norms[None], jnp.zeros((pad, channels), jnp.float32)], axis=0
    )
    summed, everywhere = small_sums(mine)
    row_norms = summed[2 * tap_count] / feature_count
    tap_grads = (
        everywhere[:, : 2 * tap_count].transpose(1, 0, 2).reshape(2, tap_count, -1) * grad_scale
    )
    return (
        gate_grad.astype(jnp.bfloat16),
        up_grad.astype(jnp.bfloat16),
        down_grad,
        row_norms,
        tap_grads,
    )


PIECES = 4
ROW_TILE = 128
SUB = 32
BLOCK = 64
LANES = 128
BF16_ROWS = 16


def cut(channels):
    tiles = channels // LANES
    sizes = [(tiles + PIECES - 1 - i) // PIECES * LANES for i in range(PIECES)]
    return [(sum(sizes[:i]), sizes[i]) for i in range(PIECES)]


def less(a, b):
    return (b - a - 1 + 4096) // 4096


def whole_kernel(
    chips,
    tps,
    scale,
    gate_ref,
    up_ref,
    gtaps_ref,
    utaps_ref,
    down_ref,
    cot_ref,
    gate_v,
    up_v,
    down_out,
    norm_v,
    tap_all,
    tap_in,
    taps_v,
    a_v,
    b_v,
    hid_t,
    cot_v,
    down_v,
    pair_send,
    pair_recv,
    rs_recv,
    rs_send,
    own_v,
    hg_v,
    edge_send,
    edge_recv,
    acc_v,
    tap_mine,
    tap_pair,
    tap_chip,
    norm_all,
    *sems,
):
    (local, z_send, z_recv, pd_send, pd_recv, pt_send, pt_recv, c_send, c_recv) = sems[:9]
    (h_send, h_recv, e_send, e_recv, tp_send, tp_recv, tz_send, tz_recv) = sems[9:17]
    (ta_send, ta_recv, n_send, n_recv) = sems[17:]
    f, q = lax.axis_index("fs"), lax.axis_index("tp")
    z, core = f // 2, f % 2
    fs = 2 * chips
    partner = z * 2 + 1 - core
    rows, features = cot_ref.shape
    channels, cols = down_ref.shape
    total_rows = rows * tps
    chip_cols = 2 * cols
    pieces = cut(channels)
    lane_tiles = channels // LANES
    half = z // (chips // 2)
    width = math.isqrt(tps)
    spot = snake(q, width)
    half_ring = tps // 2
    ring_next = (snake((spot + 1) % tps, width), snake((spot + tps - 1) % tps, width))
    f32, bf16 = jnp.float32, jnp.bfloat16

    def remote(src, dst, send, recv, device):
        return pltpu.make_async_remote_copy(
            src_ref=src,
            dst_ref=dst,
            send_sem=send,
            recv_sem=recv,
            device_id=device,
            device_id_type=MESH,
        )

    def down_piece(chip, which, s):
        col = pl.multiple_of(chip * chip_cols + which * cols, cols)
        return down_v.at[pl.ds(*pieces[s]), pl.ds(col, cols)]

    own_cot = pltpu.make_async_copy(
        cot_ref, cot_v.at[pl.ds(pl.multiple_of(q * rows, rows), rows)], local.at[0]
    )
    own_down = pltpu.make_async_copy(
        down_ref,
        down_v.at[:, pl.ds(pl.multiple_of(f * cols, cols), cols)],
        local.at[1],
    )
    load_gate = pltpu.make_async_copy(
        gate_ref, gate_v.at[pl.ds(BF16_ROWS, total_rows)], local.at[2]
    )
    load_up = pltpu.make_async_copy(up_ref, up_v.at[pl.ds(BF16_ROWS, total_rows)], local.at[3])
    tap_col = pl.ds(pl.multiple_of(q * channels, LANES), channels)
    load_taps = [
        pltpu.make_async_copy(ref.at[:, tap_col], tap_in.at[b], local.at[7 + b])
        for b, ref in enumerate((gtaps_ref, utaps_ref))
    ]
    own_down.start()
    own_cot.start()
    load_taps[0].start()
    load_taps[1].start()
    load_gate.start()
    load_up.start()

    barrier = pltpu.get_barrier_semaphore()
    for i in range(1, fs):
        pl.semaphore_signal(barrier, inc=1, device_id={"fs": (f + i) % fs}, device_id_type=MESH)
    for i in range(1, tps):
        pl.semaphore_signal(barrier, inc=1, device_id={"tp": (q + i) % tps}, device_id_type=MESH)
    for i in range(1, tps):
        pl.semaphore_signal(
            barrier,
            inc=1,
            device_id={"fs": partner, "tp": (q + i) % tps},
            device_id_type=MESH,
        )
    pl.semaphore_wait(barrier, fs + 2 * tps - 3)

    def chip_at(position, way):
        return position + way * (chips - 1 - 2 * position)

    def z_copy(src, dst, way, p, s):
        return remote(
            src,
            dst,
            z_send.at[way, p, s],
            z_recv.at[way, p, s],
            {"fs": (f + 2 * (1 - 2 * way) + fs) % fs},
        )

    def pair_down(chip, which, s):
        where = down_piece(chip, which, s)
        return remote(where, where, pd_send.at[chip, s], pd_recv.at[chip, s], {"fs": partner})

    def halo_copy(i, src, dst):
        return remote(
            src.at[pl.ds(total_rows - BF16_ROWS, BF16_ROWS)],
            dst.at[pl.ds(0, BF16_ROWS)],
            h_send.at[i],
            h_recv.at[i],
            {"fs": (f + 1) % fs},
        )

    def chunk_chip(k):
        near = z + half * (chips - 1 - 2 * z)
        if k == chips - 1:
            position = near
        else:
            far = chips - 1 - near
            first = less(k, far)
            position = first * (chips - 1 - k) + (1 - first) * (k - far)
        return position + half * (chips - 1 - 2 * position)

    def cot_part(owner_spot, way, part, k):
        owner = snake((owner_spot + 2 * tps) % tps, width)
        col = pl.ds(pl.multiple_of(chunk_chip(k) * chip_cols, chip_cols), chip_cols)
        if part:
            start = owner * rows + way * (rows // 2)
            return cot_v.at[pl.ds(pl.multiple_of(start, rows // 2), rows // 2), col]
        return cot_v.at[pl.ds(pl.multiple_of(owner * rows, rows), rows), col]

    def ring_copy(k, step, way):
        sign = 1 - 2 * way
        where = cot_part(spot - sign * (step - 1), way, step == half_ring, k)
        return remote(
            where,
            where,
            c_send.at[k, way, step - 1],
            c_recv.at[k, way, step - 1],
            {"tp": ring_next[way]},
        )

    def ring_landing(k, step, way):
        sign = 1 - 2 * way
        where = cot_part(spot - sign * step, way, step == half_ring, k)
        return remote(
            where,
            where,
            c_send.at[k, way, step - 1],
            c_recv.at[k, way, step - 1],
            {"tp": ring_next[way]},
        )

    def ring_step(k, step):
        for way in range(2):
            ring_landing(k, step, way).wait_recv()
            if step < half_ring:
                ring_copy(k, step + 1, way).start()
        if step == 1:
            for ahead in range(1 + min(k, 1), 3):
                if k + ahead < chips:
                    for way in range(2):
                        ring_copy(k + ahead, 1, way).start()

    own_down.wait()

    @pl.when(f < fs - 1)
    def _():
        halo_copy(0, gate_ref, gate_v).start()
        halo_copy(1, up_ref, up_v).start()

    for s in range(PIECES):
        where = down_piece(z, core, s)

        @pl.when(z < chips - 1)
        def _():
            z_copy(where, where, 0, 0, s).start()

        @pl.when(z > 0)
        def _():
            z_copy(where, where, 1, 0, s).start()

    own_cot.wait()
    for way in range(2):
        ring_copy(0, 1, way).start()
    for s in range(PIECES):
        pair_down(z, core, s).start()

    for b in range(2):
        load_taps[b].wait()
        taps_v[b, 0:3, :] = tap_in[b].astype(f32)

    def hidden_tile(tile, lane_tile):
        lane = pl.ds(pl.multiple_of(lane_tile * LANES, LANES), LANES)
        gt = [taps_v[0, k : k + 1, lane] for k in range(3)]
        ut = [taps_v[1, k : k + 1, lane] for k in range(3)]
        parts = []
        for i in range(ROW_TILE // SUB):
            start = pl.multiple_of(tile * ROW_TILE + i * SUB, SUB)
            window = pl.ds(start, SUB + BF16_ROWS)
            g = gate_v[window, lane].astype(f32)
            u = up_v[window, lane].astype(f32)
            g_conv = (
                gt[0] * pltpu.roll(g, 2, 0)[BF16_ROWS:]
                + gt[1] * pltpu.roll(g, 1, 0)[BF16_ROWS:]
                + gt[2] * g[BF16_ROWS:]
            )
            u_conv = (
                ut[0] * pltpu.roll(u, 2, 0)[BF16_ROWS:]
                + ut[1] * pltpu.roll(u, 1, 0)[BF16_ROWS:]
                + ut[2] * u[BF16_ROWS:]
            )
            sig = 0.5 * jnp.tanh(0.5 * g_conv) + 0.5
            act = g_conv * sig
            out = pl.ds(start, SUB)
            a_v[out, lane] = u_conv * (sig + act * (1.0 - sig))
            b_v[out, lane] = act
            parts.append((act * u_conv).astype(bf16))
        tile_t = jnp.concatenate(parts, axis=0).T
        hid_t[lane, pl.ds(pl.multiple_of(tile * ROW_TILE, ROW_TILE), ROW_TILE)] = tile_t

    tiles = total_rows // ROW_TILE

    def hidden_piece(s, first, count):
        start, size = pieces[s]
        lane_count = size // LANES

        def step(i, carry):
            hidden_tile(first + i // lane_count, start // LANES + i % lane_count)
            return carry

        lax.fori_loop(0, count * lane_count, step, 0)

    load_gate.wait()
    load_up.wait()
    hidden_piece(0, 1, tiles - 1)
    hidden_piece(1, 1, tiles - 1)

    @pl.when(f > 0)
    def _():
        halo_copy(0, gate_ref, gate_v).wait_recv()
        halo_copy(1, up_ref, up_v).wait_recv()

    @pl.when(f == 0)
    def _():
        gate_v[0:BF16_ROWS, :] = jnp.zeros((BF16_ROWS, channels), bf16)
        up_v[0:BF16_ROWS, :] = jnp.zeros((BF16_ROWS, channels), bf16)

    hidden_piece(0, 0, 1)
    hidden_piece(1, 0, 1)
    ring_step(0, 1)
    hidden_piece(2, 0, tiles)
    hidden_piece(3, 0, tiles)

    def pair_terms_copy(chip, s):
        here = pl.ds(*pieces[s])
        return remote(
            pair_send.at[chip, here],
            pair_recv.at[chip, here],
            pt_send.at[chip, s],
            pt_recv.at[chip, s],
            {"fs": partner},
        )

    def pair_terms(k):
        chip = chunk_chip(k)
        both = cot_v[:, pl.ds(pl.multiple_of(chip * chip_cols, chip_cols), chip_cols)]
        mid = PIECES // 2
        for group in (range(mid), range(mid, PIECES)):
            start = pieces[group[0]][0]
            size = sum(pieces[s][1] for s in group)
            here = pl.ds(start, size)
            value = jnp.dot(hid_t[here, :], both, preferred_element_type=f32)
            low, high = value[:, :cols], value[:, cols:]
            pair_send[chip, here, :] = jnp.where(core == 0, high, low).astype(bf16)
            for s in group:
                pair_terms_copy(chip, s).start()
            own_v[chip, here, :] = jnp.where(core == 0, low, high)

    def pair_terms_wait(k, s):
        pair_terms_copy(chunk_chip(k), s).wait_recv()

    def send_sum(position, way, p, s, first):
        chip = chip_at(chips - 1 + position - p, way)
        here = pl.ds(*pieces[s])
        value = own_v[chip, here, :] + pair_recv[chip, here, :].astype(f32)
        if not first:
            value = value + rs_recv[way, chip, here, :].astype(f32)
        rs_send[chip, here, :] = value.astype(bf16)
        z_copy(rs_send.at[chip, here], rs_recv.at[way, chip, here], way, p + 1, s).start()

    def both_ways(body):
        def step(d, carry):
            way = (half + d) % 2
            body(way, z + way * (chips - 1 - 2 * z))
            return carry

        lax.fori_loop(0, 2, step, 0)

    def first_sum(p, s):
        def body(way, position):
            @pl.when(position == 0)
            def _():
                send_sum(position, way, p, s, True)

        both_ways(body)

    def slot(p, s, arrive=True, send=True):
        here = pl.ds(*pieces[s])

        def body(way, position):
            if arrive:

                @pl.when(position > p)
                def _():
                    chip = chip_at(position - 1 - p, way)
                    where = down_piece(chip, core, s)
                    z_copy(where, where, way, p, s).wait_recv()
                    if p + 1 < chips:

                        @pl.when(position < chips - 1)
                        def _():
                            z_copy(where, where, way, p + 1, s).start()

                    pair_down(chip, core, s).start()

            if p > 0:
                if arrive:

                    @pl.when(jnp.logical_and(position > 0, position <= p))
                    def _():
                        chip = chip_at(chips - 1 + position - p, way)
                        where = rs_recv.at[way, chip, here]
                        z_copy(where, where, way, p, s).wait_recv()

                if send and p + 1 < chips:

                    @pl.when(jnp.logical_and(position > 0, position <= p))
                    def _():
                        send_sum(position, way, p, s, False)

        both_ways(body)

    def pair_down_wait(chip):
        for s in range(PIECES):
            pair_down(chip, 1 - core, s).wait_recv()

    last_chip = (1 - half) * (chips - 1)

    def hidden_grad(first_chip, count, add):
        depth = count * chip_cols
        col = pl.ds(pl.multiple_of(first_chip * chip_cols, chip_cols), depth)

        def one(start, size):
            lane = pl.ds(start, size)
            value = lax.dot_general(
                cot_v[:, col],
                down_v[lane, col],
                (((1,), (1,)), ((), ())),
                preferred_element_type=f32,
            )
            if add:
                value = value + hg_v[0:total_rows, lane]
            hg_v[0:total_rows, lane] = value

        wide = 2 * LANES

        def step(n, carry):
            one(pl.multiple_of(n * wide, wide), wide)
            return carry

        lax.fori_loop(0, channels // wide, step, 0)
        if channels % wide:
            one(channels - channels % wide, channels % wide)

    def ring_ends(k):
        for step in range(2, half_ring + 1):
            ring_step(k, step)

    def ready(k):
        ring_ends(k)
        pair_terms(k)

    def start_sums(k):
        for s in range(PIECES):
            pair_terms_wait(k, s)
            first_sum(k, s)

    mid = PIECES // 2
    for s in range(mid):
        slot(0, s)
    ready(0)
    start_sums(0)
    for s in range(mid, PIECES):
        slot(0, s)
    ring_step(1, 1)
    for p in range(1, chips - 2):
        slot(p, 0)
        ring_step(p + 1, 1)
        ring_ends(p)
        for s in range(1, mid):
            slot(p, s)
        pair_terms(p)
        start_sums(p)
        for s in range(mid, PIECES):
            slot(p, s)
    ring_step(chips - 1, 1)
    ready(chips - 2)
    for s in range(mid):
        pair_terms_wait(chips - 2, s)
    slot(chips - 2, 0)
    first_sum(chips - 2, 0)
    ready(chips - 1)
    for i in range(chips - 1):
        pair_down_wait(half + i)
    hidden_grad(half, chips - 1, False)
    for s in range(1, mid):
        first_sum(chips - 2, s)
    for s in range(PIECES):
        pair_terms_wait(chips - 1, s)
    for s in range(1, mid):
        slot(chips - 2, s)
    for s in range(mid, PIECES):
        slot(chips - 2, s, send=False)
    pair_down_wait(last_chip)
    hidden_grad(last_chip, 1, True)

    edge = 8
    row_index = lax.broadcasted_iota(jnp.int32, (edge, channels), 0)
    top = pl.ds(0, edge)
    edge_send[...] = jnp.where(
        row_index < 2,
        hg_v[top, :] * a_v[top, :],
        pltpu.roll(hg_v[top, :] * b_v[top, :], 2, 0),
    )
    edge_copy = remote(
        edge_send, edge_recv, e_send.at[0], e_recv.at[0], {"fs": (f + fs - 1) % fs}
    )

    @pl.when(f > 0)
    def _():
        edge_copy.start()

    for s in range(mid, PIECES):
        pair_terms_wait(chips - 2, s)
        first_sum(chips - 2, s)
        slot(chips - 2, s, arrive=False)

    def grads(start, lane, sums):
        window = pl.ds(start, BLOCK + edge)
        here = pl.ds(pl.multiple_of(start + BF16_ROWS, BF16_ROWS), BLOCK)
        hg = hg_v[window, lane]
        new = []
        for b, (factor, pre) in enumerate(((a_v, gate_v), (b_v, up_v))):
            g = hg * factor[window, lane]
            g0 = g[0:BLOCK]
            g1 = pltpu.roll(g, BLOCK + edge - 1, 0)[0:BLOCK]
            g2 = pltpu.roll(g, BLOCK + edge - 2, 0)[0:BLOCK]
            x = pre[here, lane].astype(f32)
            for i, shifted in enumerate((g2, g1, g0)):
                product = (shifted * x).reshape(BLOCK // 8, 8, LANES)
                new.append(sums[3 * b + i] + jnp.sum(product, axis=0))
            t = [taps_v[b, k : k + 1, lane] for k in range(3)]
            pre[here, lane] = (t[0] * g2 + t[1] * g1 + t[2] * g0).astype(bf16)
        return tuple(new)

    blocks = total_rows // BLOCK

    def grad_lanes(lane_tile, carry):
        lane = pl.ds(pl.multiple_of(lane_tile * LANES, LANES), LANES)

        def step(i, sums):
            return grads(pl.multiple_of(i * BLOCK, BLOCK), lane, sums)

        zero = jnp.zeros((8, LANES), f32)
        sums = lax.fori_loop(0, blocks - 1, step, (zero,) * 6)
        for i in range(6):
            acc_v[i, :, lane] = sums[i]
        return carry

    def grad_last(lane_tile, carry):
        lane = pl.ds(pl.multiple_of(lane_tile * LANES, LANES), LANES)
        sums = grads((blocks - 1) * BLOCK, lane, tuple(acc_v[i, :, lane] for i in range(6)))
        for b in range(2):
            for k in range(3):
                tap_mine[b, k : k + 1, lane] = jnp.sum(sums[3 * b + k], axis=0, keepdims=True)
        return carry

    lax.fori_loop(0, lane_tiles // 2, grad_lanes, 0)
    lax.fori_loop(lane_tiles // 2, lane_tiles, grad_lanes, 0)

    @pl.when(f < fs - 1)
    def _():
        edge_copy.wait_recv()

    @pl.when(f == fs - 1)
    def _():
        edge_recv[...] = jnp.zeros((edge, channels), f32)

    bottom = pl.ds(total_rows, edge)
    hg_v[bottom, :] = jnp.ones((edge, channels), f32)
    a_v[bottom, :] = edge_recv[...]
    b_v[bottom, :] = pltpu.roll(edge_recv[...], edge - 2, 0)
    tap_mine[...] = jnp.zeros(tap_mine.shape, f32)
    lax.fori_loop(0, lane_tiles, grad_last, 0)
    tap_pair_copy = remote(
        tap_mine.at[1 - core], tap_pair, tp_send.at[0], tp_recv.at[0], {"fs": partner}
    )
    tap_pair_copy.start()

    def tap_chip_copy(i, sender):
        return remote(
            tap_chip.at[sender],
            tap_chip.at[sender],
            tz_send.at[i],
            tz_recv.at[sender],
            {"fs": ((z + i) % chips) * 2 + core},
        )

    tap_pair_copy.wait_recv()
    tap_chip[z] = tap_mine[core] + tap_pair[...]
    for i in range(1, chips):
        tap_chip_copy(i, z).start()

    ones = jnp.ones((8, cols), bf16)
    contract = (((1,), (1,)), ((), ()))
    for s in range(PIECES):
        slot(chips - 1, s)
        here = pl.ds(*pieces[s])
        value = own_v[z, here, :] + pair_recv[z, here, :].astype(f32)
        value = value + jnp.where(z > 0, rs_recv[0, z, here, :].astype(f32), 0.0)
        value = value + jnp.where(z < chips - 1, rs_recv[1, z, here, :].astype(f32), 0.0)
        value = value * scale
        down_out[here, :] = value
        square = value * value
        high = square.astype(bf16)
        low = (square - high.astype(f32)).astype(bf16)
        norm = lax.dot_general(ones, high, contract, preferred_element_type=f32)
        norm = norm + lax.dot_general(ones, low, contract, preferred_element_type=f32)
        norm_all[f, :, here] = norm[0:1]

    def norm_copy(i, sender):
        return remote(
            norm_all.at[sender],
            norm_all.at[sender],
            n_send.at[i],
            n_recv.at[sender],
            {"fs": (f + i) % fs},
        )

    for i in range(1, fs):
        norm_copy(i, f).start()
    @pl.when(f < fs - 1)
    def _():
        halo_copy(0, gate_ref, gate_v).wait_send()
        halo_copy(1, up_ref, up_v).wait_send()

    @pl.when(f > 0)
    def _():
        edge_copy.wait_send()

    for k in range(chips):
        for way in range(2):
            for step in range(1, half_ring + 1):
                ring_copy(k, step, way).wait_send()
        for s in range(PIECES):
            pair_terms_copy(k, s).wait_send()
        for s in range(PIECES):
            pair_down(k, core, s).wait_send()

    for p in range(chips):
        for s in range(PIECES):
            where = rs_send.at[0, pl.ds(*pieces[s])]

            @pl.when(z < chips - 1)
            def _():
                z_copy(where, where, 0, p, s).wait_send()

            @pl.when(z > 0)
            def _():
                z_copy(where, where, 1, p, s).wait_send()

    for i in range(1, chips):
        tap_chip_copy(i, (z + i) % chips).wait_recv()
    total = tap_chip[0]
    for i in range(1, chips):
        total = total + tap_chip[i]
    tap_all[core, q] = total * scale

    def tap_all_copy(j, i, which, sender):
        to = core if j == 0 else 1 - core
        return remote(
            tap_all.at[which, sender],
            tap_all.at[which, sender],
            ta_send.at[j, i],
            ta_recv.at[which, sender],
            {"fs": z * 2 + to, "tp": (q + i) % tps},
        )

    others = [(j, i) for i in range(tps) for j in range(2) if (j, i) != (0, 0)]
    for j, i in others:
        tap_all_copy(j, i, core, q).start()
    for i in range(1, fs):
        norm_copy(i, (f + i) % fs).wait_recv()
    total = norm_all[0]
    for i in range(1, fs):
        total = total + norm_all[i]
    norm_v[...] = total * (1.0 / features)
    for j, i in others:
        which = core if j == 0 else 1 - core
        tap_all_copy(j, i, which, (q + i) % tps).wait_recv()

    tap_pair_copy.wait_send()
    for i in range(1, chips):
        tap_chip_copy(i, z).wait_send()
    for j, i in others:
        tap_all_copy(j, i, core, q).wait_send()
    for i in range(1, fs):
        norm_copy(i, f).wait_send()


def hand_over_kernel(*refs):
    gate_ref, up_ref, down_ref, norm_ref, taps_ref = refs[:5]
    gate_out, up_out, down_out, norm_out, taps_out, sems = refs[5:]
    rows = gate_out.shape[0]
    copies = [
        pltpu.make_async_copy(gate_ref.at[pl.ds(BF16_ROWS, rows)], gate_out, sems.at[0]),
        pltpu.make_async_copy(up_ref.at[pl.ds(BF16_ROWS, rows)], up_out, sems.at[1]),
        pltpu.make_async_copy(down_ref, down_out, sems.at[2]),
    ]
    for copy in copies:
        copy.start()
    channels = norm_ref.shape[1]
    norm_out[...] = norm_ref[0]
    for b in range(2):
        for k in range(3):
            for i in range(taps_ref.shape[1]):
                taps_out[k, b : b + 1, i * channels : (i + 1) * channels] = taps_ref[
                    b, i, k : k + 1, :
                ]
    for copy in copies:
        copy.wait()


def hand_over(gate_grad, up_grad, down_grad, norms, taps):
    tps, channels = taps.shape[1], taps.shape[3]
    rows = gate_grad.shape[0] - BF16_ROWS
    f32 = jnp.float32
    return pl.pallas_call(
        hand_over_kernel,
        out_shape=(
            jax.ShapeDtypeStruct((rows, channels), gate_grad.dtype),
            jax.ShapeDtypeStruct((rows, channels), gate_grad.dtype),
            jax.ShapeDtypeStruct(down_grad.shape, f32),
            jax.ShapeDtypeStruct((channels,), f32),
            jax.ShapeDtypeStruct((3, 2, channels * tps), f32),
        ),
        in_specs=[pl.BlockSpec(memory_space=pl.ANY)] * 3
        + [pl.BlockSpec(memory_space=pltpu.VMEM)] * 2,
        out_specs=[pl.BlockSpec(memory_space=pl.ANY)] * 3
        + [pl.BlockSpec(memory_space=pltpu.VMEM)] * 2,
        scratch_shapes=[pltpu.SemaphoreType.DMA((3,))],
        compiler_params=pltpu.CompilerParams(vmem_limit_bytes=2_000_000),
        name="hand_over",
    )(gate_grad, up_grad, down_grad, norms, taps)


def whole_body(gate_pre, up_pre, gate_taps, up_taps, down_proj, cotangent):
    fs, tps = lax.axis_size("fs"), lax.axis_size("tp")
    chips = fs // 2
    rows, features = cotangent.shape
    channels, cols = down_proj.shape
    total = rows * tps
    f32, bf16 = jnp.float32, jnp.bfloat16
    dma = pltpu.SemaphoreType.DMA
    scale = 1.0 / math.sqrt(total * fs)
    ring = (chips, 2, tps // 2)
    gate_grad, up_grad, down_grad, norms, taps = pl.pallas_call(
        functools.partial(whole_kernel, chips, tps, scale),
        out_shape=(
            pltpu.VMEM((total + BF16_ROWS, channels), bf16),
            pltpu.VMEM((total + BF16_ROWS, channels), bf16),
            pltpu.VMEM((channels, cols), f32),
            pltpu.VMEM((1, channels), f32),
            pltpu.VMEM((2, tps, 4, channels), f32),
        ),
        in_specs=[
            pl.BlockSpec(memory_space=pl.ANY)
        ]
        * 6,
        out_specs=[pl.BlockSpec(memory_space=pltpu.VMEM)] * 5,
        scratch_shapes=[
            pltpu.VMEM((2, 3, channels), bf16),
            pltpu.VMEM((2, 4, channels), f32),
            pltpu.VMEM((total + 8, channels), f32),
            pltpu.VMEM((total + 8, channels), f32),
            pltpu.VMEM((channels, total), bf16),
            pltpu.VMEM((total, features), bf16),
            pltpu.VMEM((channels, features), bf16),
            pltpu.VMEM((chips, channels, cols), bf16),
            pltpu.VMEM((chips, channels, cols), bf16),
            pltpu.VMEM((2, chips, channels, cols), bf16),
            pltpu.VMEM((chips, channels, cols), bf16),
            pltpu.VMEM((chips, channels, cols), f32),
            pltpu.VMEM((total + 8, channels), f32),
            pltpu.VMEM((8, channels), f32),
            pltpu.VMEM((8, channels), f32),
            pltpu.VMEM((6, 8, channels), f32),
            pltpu.VMEM((2, 4, channels), f32),
            pltpu.VMEM((4, channels), f32),
            pltpu.VMEM((chips, 4, channels), f32),
            pltpu.VMEM((fs, 1, channels), f32),
            dma((9,)),
            dma((2, chips, PIECES)),
            dma((2, chips, PIECES)),
            dma((chips, PIECES)),
            dma((chips, PIECES)),
            dma((chips, PIECES)),
            dma((chips, PIECES)),
            dma(ring),
            dma(ring),
            dma((2,)),
            dma((2,)),
            dma((1,)),
            dma((1,)),
            dma((1,)),
            dma((1,)),
            dma((chips,)),
            dma((chips,)),
            dma((2, tps)),
            dma((2, tps)),
            dma((fs,)),
            dma((fs,)),
        ],
        compiler_params=pltpu.CompilerParams(
            collective_id=2, has_side_effects=True, vmem_limit_bytes=VMEM_BYTES
        ),
        name="whole_layer",
    )(gate_pre, up_pre, gate_taps, up_taps, down_proj, cotangent)
    gate_grad, up_grad, down_grad, norms, taps = hand_over(
        gate_grad, up_grad, down_grad, norms, taps
    )
    return gate_grad, up_grad, down_grad, norms, taps.transpose(1, 0, 2)


VMEM_BYTES = 56_500_000
SPARE_BYTES = 0


def fits_whole(gate_pre, gate_taps, down_proj, cotangent):
    fs, tps = lax.axis_size("fs"), lax.axis_size("tp")
    chips = fs // 2
    channels, cols = down_proj.shape
    rows, features = cotangent.shape
    total = rows * tps
    tiled = channels % LANES == 0 and cols % (2 * LANES) == 0
    tiled = tiled and channels >= LANES * PIECES and total % ROW_TILE == 0
    tiled = tiled and rows % (2 * BF16_ROWS) == 0 and gate_taps.shape[0] == 3
    tiled = tiled and fs % 2 == 0 and chips % 2 == 0 and chips >= 4 and tps >= 4
    held = 2 * total * channels * 4 + total * channels * (2 + 4)
    held += (total + channels) * features * 2 + channels * cols * chips * (5 * 2 + 4)
    return tiled and held + SPARE_BYTES < VMEM_BYTES


def body(gate_pre, up_pre, gate_taps, up_taps, down_proj, cotangent):
    args = (gate_pre, up_pre, gate_taps, up_taps, down_proj, cotangent)
    if fits_whole(gate_pre, gate_taps, down_proj, cotangent):
        return whole_body(*args)
    return staged_body(*args)


def solution(mesh):
    placed = (P("fs", "tp"), P("fs", "tp"), P(), P(), P("tp", "fs"), P(("fs", "tp"), None))
    return jax.shard_map(
        body,
        mesh=mesh,
        in_specs=placed,
        out_specs=(P("fs", "tp"), P("fs", "tp"), P("tp", "fs"), P("tp"), P()),
        check_vma=False,
    )
```

```python
import functools
import math

import jax
import jax.numpy as jnp
from jax import lax
from jax.experimental import pallas as pl
from jax.experimental.pallas import tpu as pltpu
from jax.sharding import PartitionSpec as P

MESH = pl.DeviceIdType.MESH


def snake(position, width):
    row, column = position // width, position % width
    return row * width + column + (row % 2) * (width - 1 - 2 * column)


def gather_kernel(chips, tps, cot_ref, down_ref, cot_out, down_out, *sems):
    (ring_send, ring_recv, line_send, line_recv, pair_send, pair_recv, local_sem) = sems
    f, q = lax.axis_index("fs"), lax.axis_index("tp")
    z, core = f // 2, f % 2
    width = math.isqrt(tps)
    spot = snake(q, width)
    half_ring = tps // 2
    ring_next = (snake((spot + 1) % tps, width), snake((spot + tps - 1) % tps, width))
    rows = cot_ref.shape[0]
    cols = down_ref.shape[1]
    partner = z * 2 + 1 - core
    behind, ahead = z > 0, z < chips - 1

    barrier = pltpu.get_barrier_semaphore()
    for device in ({"tp": ring_next[0]}, {"tp": ring_next[1]}, {"fs": partner}):
        pl.semaphore_signal(barrier, inc=1, device_id=device, device_id_type=MESH)

    @pl.when(behind)
    def _():
        pl.semaphore_signal(barrier, inc=1, device_id={"fs": f - 2}, device_id_type=MESH)

    @pl.when(ahead)
    def _():
        pl.semaphore_signal(barrier, inc=1, device_id={"fs": f + 2}, device_id_type=MESH)

    pl.semaphore_wait(barrier, 4 + (z + chips - 1) // chips - (z + 1) // chips)

    def cot_rows(owner_spot, way, part):
        owner = snake((owner_spot + 2 * tps) % tps, width)
        if part:
            return pl.ds(owner * rows + way * (rows // 2), rows // 2)
        return pl.ds(owner * rows, rows)

    def ring_copy(step, way):
        sign = 1 - 2 * way
        part = step == half_ring
        where = cot_rows(spot - sign * (step - 1), way, part)
        if step == 1:
            src = cot_ref.at[pl.ds(way * (rows // 2), rows // 2)] if part else cot_ref
        else:
            src = cot_out.at[where]
        return pltpu.make_async_remote_copy(
            src_ref=src,
            dst_ref=cot_out.at[where],
            send_sem=ring_send.at[way, step - 1],
            recv_sem=ring_recv.at[way, step - 1],
            device_id={"tp": ring_next[way]},
            device_id_type=MESH,
        )

    def ring_landing(step, way):
        sign = 1 - 2 * way
        where = cot_rows(spot - sign * step, way, step == half_ring)
        return pltpu.make_async_remote_copy(
            src_ref=cot_out.at[where],
            dst_ref=cot_out.at[where],
            send_sem=ring_send.at[way, step - 1],
            recv_sem=ring_recv.at[way, step - 1],
            device_id={"tp": ring_next[way]},
            device_id_type=MESH,
        )

    def down_block(chip, which):
        block = chip * 2 + which
        if cols % 128:
            return down_out.at[block]
        return down_out.at[:, pl.ds(pl.multiple_of(block * cols, cols), cols)]

    def line_copy(step, way):
        sign = 1 - 2 * way
        where = down_block(z - sign * (step - 1), core)
        return pltpu.make_async_remote_copy(
            src_ref=down_ref if step == 1 else where,
            dst_ref=where,
            send_sem=line_send.at[way, step - 1],
            recv_sem=line_recv.at[way, step - 1],
            device_id={"fs": f + 2 * sign},
            device_id_type=MESH,
        )

    def line_landing(step, way):
        sign = 1 - 2 * way
        where = down_block(z - sign * step, core)
        return pltpu.make_async_remote_copy(
            src_ref=where,
            dst_ref=where,
            send_sem=line_send.at[way, step - 1],
            recv_sem=line_recv.at[way, step - 1],
            device_id={"fs": f + 2 * sign},
            device_id_type=MESH,
        )

    def pair_copy(step, way, which):
        sign = 1 - 2 * way
        where = down_block(z - sign * step, which)
        slot = step + way * (chips - 1)
        return pltpu.make_async_remote_copy(
            src_ref=down_ref if step == 0 else where,
            dst_ref=where,
            send_sem=pair_send.at[slot],
            recv_sem=pair_recv.at[slot],
            device_id={"fs": partner},
            device_id_type=MESH,
        )

    def has_landing(step, way):
        return z >= step if way == 0 else z + step < chips

    def has_copy(step, way):
        going = ahead if way == 0 else behind
        return going if step == 1 else jnp.logical_and(going, has_landing(step - 1, way))

    for way in range(2):
        ring_copy(1, way).start()

        @pl.when(has_copy(1, way))
        def _():
            line_copy(1, way).start()

    pair_copy(0, 0, core).start()
    own_cot = pltpu.make_async_copy(cot_ref, cot_out.at[pl.ds(q * rows, rows)], local_sem.at[0])
    own_down = pltpu.make_async_copy(down_ref, down_block(z, core), local_sem.at[1])
    own_cot.start()
    own_down.start()

    for step in range(1, max(chips - 1, half_ring) + 1):
        if step <= chips - 1:
            for way in range(2):

                @pl.when(has_landing(step, way))
                def _():
                    line_landing(step, way).wait_recv()
                    pair_copy(step, way, core).start()

                if step + 1 <= chips - 1:

                    @pl.when(has_copy(step + 1, way))
                    def _():
                        line_copy(step + 1, way).start()

        if step <= half_ring:
            for way in range(2):
                ring_landing(step, way).wait_recv()
                if step + 1 <= half_ring:
                    ring_copy(step + 1, way).start()

    own_cot.wait()
    own_down.wait()
    pair_copy(0, 0, 1 - core).wait_recv()
    pair_copy(0, 0, core).wait_send()
    for way in range(2):
        for step in range(1, half_ring + 1):
            ring_copy(step, way).wait_send()
        for step in range(1, chips):

            @pl.when(has_copy(step, way))
            def _():
                line_copy(step, way).wait_send()

            @pl.when(has_landing(step, way))
            def _():
                pair_copy(step, way, 1 - core).wait_recv()
                pair_copy(step, way, core).wait_send()


def gather_both(cotangent, down_proj):
    fs, tps = lax.axis_size("fs"), lax.axis_size("tp")
    chips = fs // 2
    rows, features = cotangent.shape
    channels, cols = down_proj.shape
    dma = pltpu.SemaphoreType.DMA
    down_shape = (fs, channels, cols) if cols % 128 else (channels, cols * fs)
    whole_cot, whole_down = pl.pallas_call(
        functools.partial(gather_kernel, chips, tps),
        out_shape=(
            jax.ShapeDtypeStruct((rows * tps, features), cotangent.dtype),
            jax.ShapeDtypeStruct(down_shape, down_proj.dtype),
        ),
        in_specs=[pl.BlockSpec(memory_space=pltpu.VMEM)] * 2,
        out_specs=[pl.BlockSpec(memory_space=pl.ANY)] * 2,
        scratch_shapes=[
            dma((2, tps // 2)),
            dma((2, tps // 2)),
            dma((2, chips - 1)),
            dma((2, chips - 1)),
            dma((2 * chips - 1,)),
            dma((2 * chips - 1,)),
            dma((2,)),
        ],
        compiler_params=pltpu.CompilerParams(collective_id=0, has_side_effects=True),
        name="gather_both",
    )(cotangent, down_proj)
    if cols % 128:
        whole_down = whole_down.transpose(1, 0, 2).reshape(channels, fs * cols)
    return whole_cot, whole_down


def small_kernel(fs, tps, mine_ref, sum_ref, all_ref, terms, total, sums, *sems):
    send_a, recv_a, send_b, recv_b = sems
    f, q = lax.axis_index("fs"), lax.axis_index("tp")
    barrier = pltpu.get_barrier_semaphore()
    for i in range(1, fs):
        pl.semaphore_signal(
            barrier, inc=1, device_id={"fs": (f + i) % fs}, device_id_type=MESH
        )
    for i in range(1, tps):
        pl.semaphore_signal(
            barrier, inc=1, device_id={"tp": (q + i) % tps}, device_id_type=MESH
        )
    pl.semaphore_wait(barrier, fs + tps - 2)

    def over_fs(i):
        return pltpu.make_async_remote_copy(
            src_ref=mine_ref,
            dst_ref=terms.at[f],
            send_sem=send_a.at[i],
            recv_sem=recv_a.at[i],
            device_id={"fs": (f + i) % fs},
            device_id_type=MESH,
        )

    def over_tp(i):
        return pltpu.make_async_remote_copy(
            src_ref=total,
            dst_ref=sums.at[q],
            send_sem=send_b.at[i],
            recv_sem=recv_b.at[i],
            device_id={"tp": (q + i) % tps},
            device_id_type=MESH,
        )

    def landing(buffer, slot, send, recv, i, device):
        return pltpu.make_async_remote_copy(
            src_ref=buffer.at[slot],
            dst_ref=buffer.at[slot],
            send_sem=send.at[i],
            recv_sem=recv.at[i],
            device_id=device,
            device_id_type=MESH,
        )

    for i in range(1, fs):
        over_fs(i).start()
    terms[f] = mine_ref[...]
    for i in range(1, fs):
        landing(terms, (f + fs - i) % fs, send_a, recv_a, i, {"fs": (f + i) % fs}).wait_recv()
    added = terms[0]
    for i in range(1, fs):
        added = added + terms[i]
    total[...] = added
    sum_ref[...] = added
    sums[q] = added
    for i in range(1, fs):
        over_fs(i).wait_send()
    for i in range(1, tps):
        over_tp(i).start()
    for i in range(1, tps):
        landing(sums, (q + tps - i) % tps, send_b, recv_b, i, {"tp": (q + i) % tps}).wait_recv()
    all_ref[...] = sums[...]
    for i in range(1, tps):
        over_tp(i).wait_send()


def small_sums(mine):
    fs, tps = lax.axis_size("fs"), lax.axis_size("tp")
    dma = pltpu.SemaphoreType.DMA
    shape = mine.shape
    return pl.pallas_call(
        functools.partial(small_kernel, fs, tps),
        out_shape=(
            jax.ShapeDtypeStruct(shape, jnp.float32),
            jax.ShapeDtypeStruct((tps,) + shape, jnp.float32),
        ),
        in_specs=[pl.BlockSpec(memory_space=pltpu.VMEM)],
        out_specs=[pl.BlockSpec(memory_space=pltpu.VMEM)] * 2,
        scratch_shapes=[
            pltpu.VMEM((fs,) + shape, jnp.float32),
            pltpu.VMEM(shape, jnp.float32),
            pltpu.VMEM((tps,) + shape, jnp.float32),
            dma((fs,)),
            dma((fs,)),
            dma((tps,)),
            dma((tps,)),
        ],
        compiler_params=pltpu.CompilerParams(collective_id=1, has_side_effects=True),
        name="small_sums",
    )(mine)


def from_behind(block, axis, distance):
    devices = range(lax.axis_size(axis))
    route = [(i - distance, i) for i in devices if i - distance in devices]
    return lax.ppermute(block, axis, route)


def staged_body(gate_pre, up_pre, gate_taps, up_taps, down_proj, cotangent):
    row_count = gate_pre.shape[0]
    channels = gate_pre.shape[1]
    tap_count = gate_taps.shape[0]
    reach = tap_count - 1
    channel_start = lax.axis_index("tp") * channels
    gate_taps_f = lax.dynamic_slice_in_dim(gate_taps, channel_start, channels, 1).astype(
        jnp.float32
    )
    up_taps_f = lax.dynamic_slice_in_dim(up_taps, channel_start, channels, 1).astype(jnp.float32)
    before = from_behind((gate_pre[row_count - reach :], up_pre[row_count - reach :]), "fs", 1)
    gate_padded = jnp.concatenate([before[0], gate_pre], axis=0).astype(jnp.float32)
    up_padded = jnp.concatenate([before[1], up_pre], axis=0).astype(jnp.float32)
    gate_conv = gate_taps_f[0] * gate_padded[0:row_count]
    up_conv = up_taps_f[0] * up_padded[0:row_count]
    for offset in range(1, tap_count):
        gate_conv = gate_conv + gate_taps_f[offset] * gate_padded[offset : offset + row_count]
        up_conv = up_conv + up_taps_f[offset] * up_padded[offset : offset + row_count]
    gate_sigmoid = jax.nn.sigmoid(gate_conv)
    gate_act = gate_conv * gate_sigmoid
    hidden = (gate_act * up_conv).astype(jnp.bfloat16)
    hidden = lax.optimization_barrier(hidden)
    whole_cot, whole_down = gather_both(cotangent, down_proj)
    grad_scale = 1.0 / math.sqrt(row_count * lax.axis_size("fs"))
    sum_type = jnp.bfloat16 if lax.axis_size("fs") <= 8 else jnp.float32
    terms = lax.dot_general(
        whole_cot, hidden, (((0,), (0,)), ((), ())), preferred_element_type=jnp.float32
    ).astype(sum_type)
    terms, whole_down = lax.optimization_barrier((terms, whole_down))
    own_rows = lax.psum_scatter(terms, "fs", scatter_dimension=0, tiled=True)
    own_rows = own_rows.astype(jnp.float32) * grad_scale
    hidden_grad = lax.dot_general(
        whole_cot,
        whole_down,
        (((1,), (1,)), ((), ())),
        preferred_element_type=jnp.float32,
    )
    gate_conv_grad = hidden_grad * up_conv * gate_sigmoid * (1.0 + gate_conv * (1.0 - gate_sigmoid))
    up_conv_grad = hidden_grad * gate_act
    following = from_behind((gate_conv_grad[0:reach], up_conv_grad[0:reach]), "fs", -1)
    gate_grad_pad = jnp.concatenate([gate_conv_grad, following[0]], axis=0)
    up_grad_pad = jnp.concatenate([up_conv_grad, following[1]], axis=0)
    gate_grad = gate_taps_f[0] * gate_grad_pad[reach : reach + row_count]
    up_grad = up_taps_f[0] * up_grad_pad[reach : reach + row_count]
    for offset in range(1, tap_count):
        lead = reach - offset
        gate_grad = gate_grad + gate_taps_f[offset] * gate_grad_pad[lead : lead + row_count]
        up_grad = up_grad + up_taps_f[offset] * up_grad_pad[lead : lead + row_count]
    gate_tap_terms = jnp.stack(
        [
            jnp.sum(gate_conv_grad * gate_padded[offset : offset + row_count], axis=0)
            for offset in range(tap_count)
        ]
    )
    up_tap_terms = jnp.stack(
        [
            jnp.sum(up_conv_grad * up_padded[offset : offset + row_count], axis=0)
            for offset in range(tap_count)
        ]
    )
    tap_terms = jnp.stack([gate_tap_terms, up_tap_terms])
    feature_count = whole_cot.shape[1]
    down_grad = own_rows.T
    partial_norms = jnp.sum(own_rows * own_rows, axis=0)
    tap_rows = tap_terms.reshape(2 * tap_count, channels)
    pad = -(2 * tap_count + 1) % 8
    mine = jnp.concatenate(
        [tap_rows, partial_norms[None], jnp.zeros((pad, channels), jnp.float32)], axis=0
    )
    summed, everywhere = small_sums(mine)
    row_norms = summed[2 * tap_count] / feature_count
    tap_grads = (
        everywhere[:, : 2 * tap_count].transpose(1, 0, 2).reshape(2, tap_count, -1) * grad_scale
    )
    return (
        gate_grad.astype(jnp.bfloat16),
        up_grad.astype(jnp.bfloat16),
        down_grad,
        row_norms,
        tap_grads,
    )


PIECES = 4
ROW_TILE = 128
SUB = 32
BLOCK = 64
LANES = 128
BF16_ROWS = 16


def cut(channels):
    tiles, most = channels // LANES - 1, PIECES - 1
    sizes = [(tiles + most - 1 - i) // most * LANES for i in range(most)] + [LANES]
    return [(sum(sizes[:i]), sizes[i]) for i in range(PIECES)]


def less(a, b):
    return (b - a - 1 + 4096) // 4096


def whole_kernel(
    chips,
    tps,
    scale,
    gate_ref,
    up_ref,
    gtaps_ref,
    utaps_ref,
    down_ref,
    cot_ref,
    gate_v,
    up_v,
    down_out,
    norm_v,
    tap_all,
    tap_in,
    taps_v,
    a_v,
    b_v,
    hid_t,
    cot_v,
    down_v,
    pair_send,
    pair_recv,
    rs_recv,
    rs_send,
    own_v,
    hg_v,
    edge_send,
    edge_recv,
    acc_v,
    tap_mine,
    tap_pair,
    tap_chip,
    norm_all,
    *sems,
):
    (local, z_send, z_recv, pd_send, pd_recv, pt_send, pt_recv, c_send, c_recv) = sems[:9]
    (h_send, h_recv, e_send, e_recv, tp_send, tp_recv, tz_send, tz_recv) = sems[9:17]
    (ta_send, ta_recv, n_send, n_recv) = sems[17:]
    f, q = lax.axis_index("fs"), lax.axis_index("tp")
    z, core = f // 2, f % 2
    fs = 2 * chips
    partner = z * 2 + 1 - core
    rows, features = cot_ref.shape
    channels, cols = down_ref.shape
    total_rows = rows * tps
    chip_cols = 2 * cols
    pieces = cut(channels)
    lane_tiles = channels // LANES
    half = z // (chips // 2)
    width = math.isqrt(tps)
    spot = snake(q, width)
    half_ring = tps // 2
    ring_next = (snake((spot + 1) % tps, width), snake((spot + tps - 1) % tps, width))
    f32, bf16 = jnp.float32, jnp.bfloat16

    def remote(src, dst, send, recv, device):
        return pltpu.make_async_remote_copy(
            src_ref=src,
            dst_ref=dst,
            send_sem=send,
            recv_sem=recv,
            device_id=device,
            device_id_type=MESH,
        )

    def down_piece(chip, which, s):
        col = pl.multiple_of(chip * chip_cols + which * cols, cols)
        return down_v.at[pl.ds(*pieces[s]), pl.ds(col, cols)]

    own_cot = pltpu.make_async_copy(
        cot_ref, cot_v.at[pl.ds(pl.multiple_of(q * rows, rows), rows)], local.at[0]
    )
    own_down = pltpu.make_async_copy(
        down_ref,
        down_v.at[:, pl.ds(pl.multiple_of(f * cols, cols), cols)],
        local.at[1],
    )
    load_gate = pltpu.make_async_copy(
        gate_ref, gate_v.at[pl.ds(BF16_ROWS, total_rows)], local.at[2]
    )
    load_up = pltpu.make_async_copy(up_ref, up_v.at[pl.ds(BF16_ROWS, total_rows)], local.at[3])
    tap_col = pl.ds(pl.multiple_of(q * channels, LANES), channels)
    load_taps = [
        pltpu.make_async_copy(ref.at[:, tap_col], tap_in.at[b], local.at[7 + b])
        for b, ref in enumerate((gtaps_ref, utaps_ref))
    ]
    own_down.start()
    own_cot.start()
    load_taps[0].start()
    load_taps[1].start()
    load_gate.start()
    load_up.start()

    barrier = pltpu.get_barrier_semaphore()
    for i in range(1, fs):
        pl.semaphore_signal(barrier, inc=1, device_id={"fs": (f + i) % fs}, device_id_type=MESH)
    for i in range(1, tps):
        pl.semaphore_signal(barrier, inc=1, device_id={"tp": (q + i) % tps}, device_id_type=MESH)
    for i in range(1, tps):
        pl.semaphore_signal(
            barrier,
            inc=1,
            device_id={"fs": partner, "tp": (q + i) % tps},
            device_id_type=MESH,
        )
    pl.semaphore_wait(barrier, fs + 2 * tps - 3)

    def chip_at(position, way):
        return position + way * (chips - 1 - 2 * position)

    def z_copy(src, dst, way, p, s):
        return remote(
            src,
            dst,
            z_send.at[way, p, s],
            z_recv.at[way, p, s],
            {"fs": (f + 2 * (1 - 2 * way) + fs) % fs},
        )

    def pair_down(chip, which, s):
        where = down_piece(chip, which, s)
        return remote(where, where, pd_send.at[chip, s], pd_recv.at[chip, s], {"fs": partner})

    def halo_copy(i, src, dst):
        return remote(
            src.at[pl.ds(total_rows - BF16_ROWS, BF16_ROWS)],
            dst.at[pl.ds(0, BF16_ROWS)],
            h_send.at[i],
            h_recv.at[i],
            {"fs": (f + 1) % fs},
        )

    def chunk_chip(k):
        near = z + half * (chips - 1 - 2 * z)
        if k == chips - 1:
            position = near
        else:
            far = chips - 1 - near
            first = less(k, far)
            position = first * (chips - 1 - k) + (1 - first) * (k - far)
        return position + half * (chips - 1 - 2 * position)

    def cot_part(owner_spot, way, part, k):
        owner = snake((owner_spot + 2 * tps) % tps, width)
        col = pl.ds(pl.multiple_of(chunk_chip(k) * chip_cols, chip_cols), chip_cols)
        if part:
            start = owner * rows + way * (rows // 2)
            return cot_v.at[pl.ds(pl.multiple_of(start, rows // 2), rows // 2), col]
        return cot_v.at[pl.ds(pl.multiple_of(owner * rows, rows), rows), col]

    def ring_copy(k, step, way):
        sign = 1 - 2 * way
        where = cot_part(spot - sign * (step - 1), way, step == half_ring, k)
        return remote(
            where,
            where,
            c_send.at[k, way, step - 1],
            c_recv.at[k, way, step - 1],
            {"tp": ring_next[way]},
        )

    def ring_landing(k, step, way):
        sign = 1 - 2 * way
        where = cot_part(spot - sign * step, way, step == half_ring, k)
        return remote(
            where,
            where,
            c_send.at[k, way, step - 1],
            c_recv.at[k, way, step - 1],
            {"tp": ring_next[way]},
        )

    def ring_step(k, step):
        for way in range(2):
            ring_landing(k, step, way).wait_recv()
            if step < half_ring:
                ring_copy(k, step + 1, way).start()
        if step == 1:
            for ahead in range(1 + min(k, 1), 3):
                if k + ahead < chips:
                    for way in range(2):
                        ring_copy(k + ahead, 1, way).start()

    own_down.wait()

    @pl.when(f < fs - 1)
    def _():
        halo_copy(0, gate_ref, gate_v).start()
        halo_copy(1, up_ref, up_v).start()

    for s in range(PIECES):
        where = down_piece(z, core, s)

        @pl.when(z < chips - 1)
        def _():
            z_copy(where, where, 0, 0, s).start()

        @pl.when(z > 0)
        def _():
            z_copy(where, where, 1, 0, s).start()

    own_cot.wait()
    for way in range(2):
        ring_copy(0, 1, way).start()
    for s in range(PIECES):
        pair_down(z, core, s).start()

    for b in range(2):
        load_taps[b].wait()
        taps_v[b, 0:3, :] = tap_in[b].astype(f32)

    def hidden_tile(tile, lane_tile):
        lane = pl.ds(pl.multiple_of(lane_tile * LANES, LANES), LANES)
        gt = [taps_v[0, k : k + 1, lane] for k in range(3)]
        ut = [taps_v[1, k : k + 1, lane] for k in range(3)]
        parts = []
        for i in range(ROW_TILE // SUB):
            start = pl.multiple_of(tile * ROW_TILE + i * SUB, SUB)
            window = pl.ds(start, SUB + BF16_ROWS)
            g = gate_v[window, lane].astype(f32)
            u = up_v[window, lane].astype(f32)
            g_conv = (
                gt[0] * pltpu.roll(g, 2, 0)[BF16_ROWS:]
                + gt[1] * pltpu.roll(g, 1, 0)[BF16_ROWS:]
                + gt[2] * g[BF16_ROWS:]
            )
            u_conv = (
                ut[0] * pltpu.roll(u, 2, 0)[BF16_ROWS:]
                + ut[1] * pltpu.roll(u, 1, 0)[BF16_ROWS:]
                + ut[2] * u[BF16_ROWS:]
            )
            sig = 0.5 * jnp.tanh(0.5 * g_conv) + 0.5
            act = g_conv * sig
            out = pl.ds(start, SUB)
            a_v[out, lane] = u_conv * (sig + act * (1.0 - sig))
            b_v[out, lane] = act
            parts.append((act * u_conv).astype(bf16))
        tile_t = jnp.concatenate(parts, axis=0).T
        hid_t[lane, pl.ds(pl.multiple_of(tile * ROW_TILE, ROW_TILE), ROW_TILE)] = tile_t

    tiles = total_rows // ROW_TILE

    def hidden_piece(s, first, count):
        start, size = pieces[s]
        lane_count = size // LANES

        def step(i, carry):
            hidden_tile(first + i // lane_count, start // LANES + i % lane_count)
            return carry

        lax.fori_loop(0, count * lane_count, step, 0)

    load_gate.wait()
    load_up.wait()
    hidden_piece(0, 1, tiles - 1)
    hidden_piece(1, 1, tiles - 1)

    @pl.when(f > 0)
    def _():
        halo_copy(0, gate_ref, gate_v).wait_recv()
        halo_copy(1, up_ref, up_v).wait_recv()

    @pl.when(f == 0)
    def _():
        gate_v[0:BF16_ROWS, :] = jnp.zeros((BF16_ROWS, channels), bf16)
        up_v[0:BF16_ROWS, :] = jnp.zeros((BF16_ROWS, channels), bf16)

    hidden_piece(0, 0, 1)
    hidden_piece(1, 0, 1)
    ring_step(0, 1)
    hidden_piece(2, 0, tiles)
    hidden_piece(3, 0, tiles)

    def pair_terms_copy(chip, s):
        here = pl.ds(*pieces[s])
        return remote(
            pair_send.at[chip, here],
            pair_recv.at[chip, here],
            pt_send.at[chip, s],
            pt_recv.at[chip, s],
            {"fs": partner},
        )

    def pair_terms(k):
        chip = chunk_chip(k)
        both = cot_v[:, pl.ds(pl.multiple_of(chip * chip_cols, chip_cols), chip_cols)]
        mid = PIECES // 2
        for group in (range(mid), range(mid, PIECES)):
            start = pieces[group[0]][0]
            size = sum(pieces[s][1] for s in group)
            here = pl.ds(start, size)
            value = jnp.dot(hid_t[here, :], both, preferred_element_type=f32)
            low, high = value[:, :cols], value[:, cols:]
            pair_send[chip, here, :] = jnp.where(core == 0, high, low).astype(bf16)
            for s in group:
                pair_terms_copy(chip, s).start()
            own_v[chip, here, :] = jnp.where(core == 0, low, high)

    def pair_terms_wait(k, s):
        pair_terms_copy(chunk_chip(k), s).wait_recv()

    def send_sum(position, way, p, s, first):
        chip = chip_at(chips - 1 + position - p, way)
        here = pl.ds(*pieces[s])
        value = own_v[chip, here, :] + pair_recv[chip, here, :].astype(f32)
        if not first:
            value = value + rs_recv[way, chip, here, :].astype(f32)
        rs_send[chip, here, :] = value.astype(bf16)
        z_copy(rs_send.at[chip, here], rs_recv.at[way, chip, here], way, p + 1, s).start()

    def both_ways(body):
        def step(d, carry):
            way = (half + d) % 2
            body(way, z + way * (chips - 1 - 2 * z))
            return carry

        lax.fori_loop(0, 2, step, 0)

    def first_sum(p, s):
        def body(way, position):
            @pl.when(position == 0)
            def _():
                send_sum(position, way, p, s, True)

        both_ways(body)

    def slot(p, s, arrive=True, send=True):
        here = pl.ds(*pieces[s])

        def body(way, position):
            if arrive:

                @pl.when(position > p)
                def _():
                    chip = chip_at(position - 1 - p, way)
                    where = down_piece(chip, core, s)
                    z_copy(where, where, way, p, s).wait_recv()
                    if p + 1 < chips:

                        @pl.when(position < chips - 1)
                        def _():
                            z_copy(where, where, way, p + 1, s).start()

                    pair_down(chip, core, s).start()

            if p > 0:
                if arrive:

                    @pl.when(jnp.logical_and(position > 0, position <= p))
                    def _():
                        chip = chip_at(chips - 1 + position - p, way)
                        where = rs_recv.at[way, chip, here]
                        z_copy(where, where, way, p, s).wait_recv()

                if send and p + 1 < chips:

                    @pl.when(jnp.logical_and(position > 0, position <= p))
                    def _():
                        send_sum(position, way, p, s, False)

        both_ways(body)

    def pair_down_wait(chip, one=None):
        for s in range(PIECES) if one is None else (one,):
            pair_down(chip, 1 - core, s).wait_recv()

    last_chip = (1 - half) * (chips - 1)

    def hidden_grad(first_chip, count, add, tile_from=0, tile_to=None):
        depth = count * chip_cols
        col = pl.ds(pl.multiple_of(first_chip * chip_cols, chip_cols), depth)

        def one(start, size):
            lane = pl.ds(start, size)
            value = lax.dot_general(
                cot_v[:, col],
                down_v[lane, col],
                (((1,), (1,)), ((), ())),
                preferred_element_type=f32,
            )
            if add:
                value = value + hg_v[0:total_rows, lane]
            hg_v[0:total_rows, lane] = value

        wide = 2 * LANES

        def step(n, carry):
            one(pl.multiple_of(n * wide, wide), wide)
            return carry

        whole = channels // wide
        lax.fori_loop(tile_from, whole if tile_to is None else tile_to, step, 0)
        if channels % wide and tile_to is None:
            one(whole * wide, channels % wide)

    def ring_ends(k):
        for step in range(2, half_ring + 1):
            ring_step(k, step)

    def ready(k):
        ring_ends(k)
        pair_terms(k)

    def start_sums(k):
        for s in range(PIECES):
            pair_terms_wait(k, s)
            first_sum(k, s)

    mid = PIECES // 2
    for s in range(mid):
        slot(0, s)
    ready(0)
    start_sums(0)
    for s in range(mid, PIECES):
        slot(0, s)
    ring_step(1, 1)
    for p in range(1, chips - 2):
        slot(p, 0)
        ring_step(p + 1, 1)
        ring_ends(p)
        for s in range(1, mid):
            slot(p, s)
        pair_terms(p)
        start_sums(p)
        for s in range(mid, PIECES):
            slot(p, s)
    ring_step(chips - 1, 1)
    second_chip = (1 - half) * (chips - 2) + half
    pair_down_wait(second_chip)
    hidden_grad(second_chip, 1, False)
    ready(chips - 2)
    for s in range(mid):
        pair_terms_wait(chips - 2, s)
    slot(chips - 2, 0)
    first_sum(chips - 2, 0)
    ready(chips - 1)
    for i in range(chips - 2):
        pair_down_wait(2 * half + i)
    hidden_grad(2 * half, chips - 2, True)
    for s in range(1, mid):
        first_sum(chips - 2, s)
    for s in range(PIECES):
        pair_terms_wait(chips - 1, s)
    for s in range(1, mid):
        slot(chips - 2, s)
    for s in range(mid, PIECES - 1):
        slot(chips - 2, s, send=False)
    for s in range(PIECES - 1):
        pair_down_wait(last_chip, s)
    edge = 8

    def grads(start, lane, sums):
        window = pl.ds(start, BLOCK + edge)
        here = pl.ds(pl.multiple_of(start + BF16_ROWS, BF16_ROWS), BLOCK)
        hg = hg_v[window, lane]
        new = []
        for b, (factor, pre) in enumerate(((a_v, gate_v), (b_v, up_v))):
            g = hg * factor[window, lane]
            g0 = g[0:BLOCK]
            g1 = pltpu.roll(g, BLOCK + edge - 1, 0)[0:BLOCK]
            g2 = pltpu.roll(g, BLOCK + edge - 2, 0)[0:BLOCK]
            x = pre[here, lane].astype(f32)
            for i, shifted in enumerate((g2, g1, g0)):
                product = (shifted * x).reshape(BLOCK // 8, 8, LANES)
                new.append(sums[3 * b + i] + jnp.sum(product, axis=0))
            t = [taps_v[b, k : k + 1, lane] for k in range(3)]
            pre[here, lane] = (t[0] * g2 + t[1] * g1 + t[2] * g0).astype(bf16)
        return tuple(new)

    blocks = total_rows // BLOCK

    def grad_lanes(lane_tile, carry):
        lane = pl.ds(pl.multiple_of(lane_tile * LANES, LANES), LANES)

        def step(i, sums):
            return grads(pl.multiple_of(i * BLOCK, BLOCK), lane, sums)

        zero = jnp.zeros((8, LANES), f32)
        sums = lax.fori_loop(0, blocks - 1, step, (zero,) * 6)
        for i in range(6):
            acc_v[i, :, lane] = sums[i]
        return carry

    def grad_last(lane_tile, carry):
        lane = pl.ds(pl.multiple_of(lane_tile * LANES, LANES), LANES)
        sums = grads((blocks - 1) * BLOCK, lane, tuple(acc_v[i, :, lane] for i in range(6)))
        for b in range(2):
            for k in range(3):
                tap_mine[b, k : k + 1, lane] = jnp.sum(sums[3 * b + k], axis=0, keepdims=True)
        return carry

    def grad_range(first, last):
        lax.fori_loop(first, last, grad_lanes, 0)

    early_tiles = pieces[-1][0] // (2 * LANES)
    hidden_grad(last_chip, 1, True, 0, early_tiles)
    grad_range(0, lane_tiles // 4)
    slot(chips - 2, PIECES - 1, send=False)
    grad_range(lane_tiles // 4, lane_tiles // 2)
    pair_down_wait(last_chip, PIECES - 1)
    hidden_grad(last_chip, 1, True, early_tiles)

    row_index = lax.broadcasted_iota(jnp.int32, (edge, channels), 0)
    top = pl.ds(0, edge)
    edge_send[...] = jnp.where(
        row_index < 2,
        hg_v[top, :] * a_v[top, :],
        pltpu.roll(hg_v[top, :] * b_v[top, :], 2, 0),
    )
    edge_copy = remote(
        edge_send, edge_recv, e_send.at[0], e_recv.at[0], {"fs": (f + fs - 1) % fs}
    )

    @pl.when(f > 0)
    def _():
        edge_copy.start()

    for s in range(mid, PIECES):
        pair_terms_wait(chips - 2, s)
    for s in range(mid, PIECES - 1):
        first_sum(chips - 2, s)
        slot(chips - 2, s, arrive=False)

    grad_range(lane_tiles // 2, lane_tiles)

    @pl.when(f < fs - 1)
    def _():
        edge_copy.wait_recv()

    @pl.when(f == fs - 1)
    def _():
        edge_recv[...] = jnp.zeros((edge, channels), f32)

    bottom = pl.ds(total_rows, edge)
    hg_v[bottom, :] = jnp.ones((edge, channels), f32)
    a_v[bottom, :] = edge_recv[...]
    b_v[bottom, :] = pltpu.roll(edge_recv[...], edge - 2, 0)
    tap_mine[...] = jnp.zeros(tap_mine.shape, f32)
    lax.fori_loop(0, lane_tiles, grad_last, 0)
    tap_pair_copy = remote(
        tap_mine.at[1 - core], tap_pair, tp_send.at[0], tp_recv.at[0], {"fs": partner}
    )
    tap_pair_copy.start()

    def tap_chip_copy(i, sender):
        return remote(
            tap_chip.at[sender],
            tap_chip.at[sender],
            tz_send.at[i],
            tz_recv.at[sender],
            {"fs": ((z + i) % chips) * 2 + core},
        )

    tap_pair_copy.wait_recv()
    tap_chip[z] = tap_mine[core] + tap_pair[...]
    for i in range(1, chips):
        tap_chip_copy(i, z).start()
    first_sum(chips - 2, PIECES - 1)
    slot(chips - 2, PIECES - 1, arrive=False)

    ones = jnp.ones((8, cols), bf16)
    contract = (((1,), (1,)), ((), ()))
    for s in range(PIECES):
        slot(chips - 1, s)
        here = pl.ds(*pieces[s])
        value = own_v[z, here, :] + pair_recv[z, here, :].astype(f32)
        value = value + jnp.where(z > 0, rs_recv[0, z, here, :].astype(f32), 0.0)
        value = value + jnp.where(z < chips - 1, rs_recv[1, z, here, :].astype(f32), 0.0)
        value = value * scale
        down_out[here, :] = value
        square = value * value
        high = square.astype(bf16)
        low = (square - high.astype(f32)).astype(bf16)
        norm = lax.dot_general(ones, high, contract, preferred_element_type=f32)
        norm = norm + lax.dot_general(ones, low, contract, preferred_element_type=f32)
        norm_all[f, :, here] = norm[0:1]

    def norm_copy(i, sender):
        return remote(
            norm_all.at[sender],
            norm_all.at[sender],
            n_send.at[i],
            n_recv.at[sender],
            {"fs": (f + i) % fs},
        )

    for i in range(1, fs):
        norm_copy(i, f).start()
    @pl.when(f < fs - 1)
    def _():
        halo_copy(0, gate_ref, gate_v).wait_send()
        halo_copy(1, up_ref, up_v).wait_send()

    @pl.when(f > 0)
    def _():
        edge_copy.wait_send()

    for k in range(chips):
        for way in range(2):
            for step in range(1, half_ring + 1):
                ring_copy(k, step, way).wait_send()
        for s in range(PIECES):
            pair_terms_copy(k, s).wait_send()
        for s in range(PIECES):
            pair_down(k, core, s).wait_send()

    for p in range(chips):
        for s in range(PIECES):
            where = rs_send.at[0, pl.ds(*pieces[s])]

            @pl.when(z < chips - 1)
            def _():
                z_copy(where, where, 0, p, s).wait_send()

            @pl.when(z > 0)
            def _():
                z_copy(where, where, 1, p, s).wait_send()

    for i in range(1, chips):
        tap_chip_copy(i, (z + i) % chips).wait_recv()
    total = tap_chip[0]
    for i in range(1, chips):
        total = total + tap_chip[i]
    tap_all[core, q] = total * scale

    def tap_all_copy(j, i, which, sender):
        to = core if j == 0 else 1 - core
        return remote(
            tap_all.at[which, sender],
            tap_all.at[which, sender],
            ta_send.at[j, i],
            ta_recv.at[which, sender],
            {"fs": z * 2 + to, "tp": (q + i) % tps},
        )

    others = [(j, i) for i in range(tps) for j in range(2) if (j, i) != (0, 0)]
    for j, i in others:
        tap_all_copy(j, i, core, q).start()
    for i in range(1, fs):
        norm_copy(i, (f + i) % fs).wait_recv()
    total = norm_all[0]
    for i in range(1, fs):
        total = total + norm_all[i]
    norm_v[...] = total * (1.0 / features)
    for j, i in others:
        which = core if j == 0 else 1 - core
        tap_all_copy(j, i, which, (q + i) % tps).wait_recv()

    tap_pair_copy.wait_send()
    for i in range(1, chips):
        tap_chip_copy(i, z).wait_send()
    for j, i in others:
        tap_all_copy(j, i, core, q).wait_send()
    for i in range(1, fs):
        norm_copy(i, f).wait_send()


def hand_over_kernel(*refs):
    gate_ref, up_ref, down_ref, norm_ref, taps_ref = refs[:5]
    gate_out, up_out, down_out, norm_out, taps_out, sems = refs[5:]
    rows = gate_out.shape[0]
    copies = [
        pltpu.make_async_copy(gate_ref.at[pl.ds(BF16_ROWS, rows)], gate_out, sems.at[0]),
        pltpu.make_async_copy(up_ref.at[pl.ds(BF16_ROWS, rows)], up_out, sems.at[1]),
        pltpu.make_async_copy(down_ref, down_out, sems.at[2]),
    ]
    for copy in copies:
        copy.start()
    channels = norm_ref.shape[1]
    norm_out[...] = norm_ref[0]
    for b in range(2):
        for k in range(3):
            for i in range(taps_ref.shape[1]):
                taps_out[k, b : b + 1, i * channels : (i + 1) * channels] = taps_ref[
                    b, i, k : k + 1, :
                ]
    for copy in copies:
        copy.wait()


def hand_over(gate_grad, up_grad, down_grad, norms, taps):
    tps, channels = taps.shape[1], taps.shape[3]
    rows = gate_grad.shape[0] - BF16_ROWS
    f32 = jnp.float32
    return pl.pallas_call(
        hand_over_kernel,
        out_shape=(
            jax.ShapeDtypeStruct((rows, channels), gate_grad.dtype),
            jax.ShapeDtypeStruct((rows, channels), gate_grad.dtype),
            jax.ShapeDtypeStruct(down_grad.shape, f32),
            jax.ShapeDtypeStruct((channels,), f32),
            jax.ShapeDtypeStruct((3, 2, channels * tps), f32),
        ),
        in_specs=[pl.BlockSpec(memory_space=pl.ANY)] * 3
        + [pl.BlockSpec(memory_space=pltpu.VMEM)] * 2,
        out_specs=[pl.BlockSpec(memory_space=pl.ANY)] * 3
        + [pl.BlockSpec(memory_space=pltpu.VMEM)] * 2,
        scratch_shapes=[pltpu.SemaphoreType.DMA((3,))],
        compiler_params=pltpu.CompilerParams(vmem_limit_bytes=2_000_000),
        name="hand_over",
    )(gate_grad, up_grad, down_grad, norms, taps)


def whole_body(gate_pre, up_pre, gate_taps, up_taps, down_proj, cotangent):
    fs, tps = lax.axis_size("fs"), lax.axis_size("tp")
    chips = fs // 2
    rows, features = cotangent.shape
    channels, cols = down_proj.shape
    total = rows * tps
    f32, bf16 = jnp.float32, jnp.bfloat16
    dma = pltpu.SemaphoreType.DMA
    scale = 1.0 / math.sqrt(total * fs)
    ring = (chips, 2, tps // 2)
    gate_grad, up_grad, down_grad, norms, taps = pl.pallas_call(
        functools.partial(whole_kernel, chips, tps, scale),
        out_shape=(
            pltpu.VMEM((total + BF16_ROWS, channels), bf16),
            pltpu.VMEM((total + BF16_ROWS, channels), bf16),
            pltpu.VMEM((channels, cols), f32),
            pltpu.VMEM((1, channels), f32),
            pltpu.VMEM((2, tps, 4, channels), f32),
        ),
        in_specs=[
            pl.BlockSpec(memory_space=pl.ANY)
        ]
        * 6,
        out_specs=[pl.BlockSpec(memory_space=pltpu.VMEM)] * 5,
        scratch_shapes=[
            pltpu.VMEM((2, 3, channels), bf16),
            pltpu.VMEM((2, 4, channels), f32),
            pltpu.VMEM((total + 8, channels), f32),
            pltpu.VMEM((total + 8, channels), f32),
            pltpu.VMEM((channels, total), bf16),
            pltpu.VMEM((total, features), bf16),
            pltpu.VMEM((channels, features), bf16),
            pltpu.VMEM((chips, channels, cols), bf16),
            pltpu.VMEM((chips, channels, cols), bf16),
            pltpu.VMEM((2, chips, channels, cols), bf16),
            pltpu.VMEM((chips, channels, cols), bf16),
            pltpu.VMEM((chips, channels, cols), f32),
            pltpu.VMEM((total + 8, channels), f32),
            pltpu.VMEM((8, channels), f32),
            pltpu.VMEM((8, channels), f32),
            pltpu.VMEM((6, 8, channels), f32),
            pltpu.VMEM((2, 4, channels), f32),
            pltpu.VMEM((4, channels), f32),
            pltpu.VMEM((chips, 4, channels), f32),
            pltpu.VMEM((fs, 1, channels), f32),
            dma((9,)),
            dma((2, chips, PIECES)),
            dma((2, chips, PIECES)),
            dma((chips, PIECES)),
            dma((chips, PIECES)),
            dma((chips, PIECES)),
            dma((chips, PIECES)),
            dma(ring),
            dma(ring),
            dma((2,)),
            dma((2,)),
            dma((1,)),
            dma((1,)),
            dma((1,)),
            dma((1,)),
            dma((chips,)),
            dma((chips,)),
            dma((2, tps)),
            dma((2, tps)),
            dma((fs,)),
            dma((fs,)),
        ],
        compiler_params=pltpu.CompilerParams(
            collective_id=2, has_side_effects=True, vmem_limit_bytes=VMEM_BYTES
        ),
        name="whole_layer",
    )(gate_pre, up_pre, gate_taps, up_taps, down_proj, cotangent)
    gate_grad, up_grad, down_grad, norms, taps = hand_over(
        gate_grad, up_grad, down_grad, norms, taps
    )
    return gate_grad, up_grad, down_grad, norms, taps.transpose(1, 0, 2)


VMEM_BYTES = 56_500_000
SPARE_BYTES = 0


def fits_whole(gate_pre, gate_taps, down_proj, cotangent):
    fs, tps = lax.axis_size("fs"), lax.axis_size("tp")
    chips = fs // 2
    channels, cols = down_proj.shape
    rows, features = cotangent.shape
    total = rows * tps
    tiled = channels % LANES == 0 and cols % (2 * LANES) == 0
    tiled = tiled and channels >= LANES * PIECES and total % ROW_TILE == 0
    tiled = tiled and rows % (2 * BF16_ROWS) == 0 and gate_taps.shape[0] == 3
    tiled = tiled and fs % 2 == 0 and chips % 2 == 0 and chips >= 4 and tps >= 4
    held = 2 * total * channels * 4 + total * channels * (2 + 4)
    held += (total + channels) * features * 2 + channels * cols * chips * (5 * 2 + 4)
    return tiled and held + SPARE_BYTES < VMEM_BYTES


def body(gate_pre, up_pre, gate_taps, up_taps, down_proj, cotangent):
    args = (gate_pre, up_pre, gate_taps, up_taps, down_proj, cotangent)
    if fits_whole(gate_pre, gate_taps, down_proj, cotangent):
        return whole_body(*args)
    return staged_body(*args)


def solution(mesh):
    placed = (P("fs", "tp"), P("fs", "tp"), P(), P(), P("tp", "fs"), P(("fs", "tp"), None))
    return jax.shard_map(
        body,
        mesh=mesh,
        in_specs=placed,
        out_specs=(P("fs", "tp"), P("fs", "tp"), P("tp", "fs"), P("tp"), P()),
        check_vma=False,
    )
```
